32 devices in a mesh: sp: 8 (over z, x), tp: 4 (over y, core).
Axes of the slice: x: 2, y: 2, z: 4, core: 2. Of those that a mesh axis runs over, the one named last changes fastest.
Arguments:
- residual: bfloat16 [4096, 2048], P('sp', 'tp'), may hold values from -64 to 64
- gains: float32 [2, 2, 2048], replicated, may hold values from 0.1 to 1.9
- w_query: bfloat16 [2, 2048, 2048], P(None, None, 'tp'), may hold values from -0.125 to 0.125
- w_key: bfloat16 [2, 2048, 2048], P(None, None, 'tp'), may hold values from -0.125 to 0.125
- w_value: bfloat16 [2, 2048, 2048], P(None, None, 'tp'), may hold values from -0.125 to 0.125
- w_out: bfloat16 [2, 2048, 2048], P(None, None, 'tp'), may hold values from -1 to 1
- rel_bias: float32 [2, 32, 257], P(None, 'tp'), may hold values from -6 to 300
Outputs:
- encoded: bfloat16 [4096, 2048], P('sp', 'tp')
The draws below stay inside these ranges and needn't reach their ends.
All inputs are finite; a program needn't handle non-finite values.
Results may differ from the reference program's by a relative error of at most 0.0058.
Values may be sent and summed in bfloat16 or wider, within the bound.
A program may use at most 128 MiB of HBM per device.

```python
import jax
import jax.numpy as jnp
from jax import lax

D = 2048
HEADS = 32
HEAD = 64
SEG = 64
LEFT = 8
MAXREL = 128
NREL = 257
LAYERS = 2
TOKENS = 4096


def rough_columns(key, col_count, rise_top):
    spread = jax.random.uniform(key, (col_count,), jnp.float32, -1.0, 1.0)
    ramp = jnp.arange(col_count, dtype=jnp.float32) / col_count
    return rise_top ** ramp * 2.0 ** spread


def draw_residual(key, part):
    key_base, key_rows, key_cols = jax.random.split(jax.random.fold_in(key, 11), 3)
    base = jnp.clip(jax.random.normal(key_base, (TOKENS, D), jnp.float32), -5.0, 5.0)
    row_scale = 0.3 * 10.0 ** jax.random.uniform(key_rows, (TOKENS, 1), jnp.float32)
    col_scale = rough_columns(key_cols, D, 3.0)
    return jnp.clip(base * row_scale * col_scale, -64.0, 64.0).astype(jnp.bfloat16)


def draw_w_out(key, part):
    key_base, key_cols = jax.random.split(jax.random.fold_in(key, 23), 2)
    base = jnp.clip(jax.random.normal(key_base, (LAYERS, D, D), jnp.float32), -5.0, 5.0)
    col_scale = rough_columns(key_cols, D, 3.0)
    scaled = base * col_scale / jnp.sqrt(jnp.float32(D))
    return jnp.clip(scaled, -1.0, 1.0).astype(jnp.bfloat16)


def draw_rel_bias(key, part):
    key_base = jax.random.fold_in(jax.random.fold_in(key, 37), 0)
    base = jnp.clip(jax.random.normal(key_base, (LAYERS, HEADS, NREL), jnp.float32), -6.0, 6.0)
    return base


def block_levels(stream_key, shape, shards, low, largest):
    loudness = 1.0
    for position, parts in shards:
        draws = jax.random.uniform(jax.random.fold_in(jax.random.fold_in(stream_key, 6), position), (parts,), jnp.float32, low / len(shards), largest / len(shards))
        loudness = loudness * jnp.repeat(jnp.exp(draws), shape[position] // parts).reshape((-1,) + (1,) * (len(shape) - 1 - position))
    return loudness


def gaussian(key, dims, scale, most, cuts=(), kind=jnp.bfloat16):
    factor_of = block_levels(key, dims, cuts, -0.22, 0.18) if cuts else 1.0
    values = jax.random.normal(key, dims, jnp.float32) * scale * factor_of
    return jnp.minimum(jnp.maximum(values, -most), most).astype(kind)


def setup_inputs(seed: int = 0) -> dict:
    keys = jax.random.split(jax.random.key(seed), 8)
    return {
        "residual": draw_residual(jax.random.fold_in(keys[7], 71), 0),
        "gains": jnp.clip(1.0 + 0.18 * jax.random.normal(keys[1], (LAYERS, 2, D), jnp.float32), 0.1, 1.9),
        "w_query": gaussian(keys[2], (LAYERS, D, D), D ** -0.5, 0.125, ((2, 4),)),
        "w_key": gaussian(keys[3], (LAYERS, D, D), D ** -0.5, 0.125, ((2, 4),)),
        "w_value": gaussian(keys[4], (LAYERS, D, D), D ** -0.5, 0.125, ((2, 4),)),
        "w_out": draw_w_out(jax.random.fold_in(keys[7], 71), 0),
        "rel_bias": draw_rel_bias(jax.random.fold_in(keys[7], 71), 0),
    }


norm_eps = 1e-06

def norm_rows(values, gain):
    widened = values.astype(jnp.float32)
    inv_rms = lax.rsqrt(lax.optimization_barrier(jnp.mean(widened * widened, axis=1, keepdims=True)) + norm_eps)
    return widened * inv_rms * gain

def attend_all(queries, key_rows, value_rows, bias_table):
    reach_rows = LEFT * SEG
    key_span = reach_rows + 128
    sub_count = queries.shape[0] // 128
    padding = jnp.zeros((reach_rows, key_rows.shape[1]), jnp.bfloat16)
    key_pad = jnp.concatenate([padding, key_rows], axis=0)
    value_pad = jnp.concatenate([padding, value_rows], axis=0)
    row_idx = jnp.arange(128, dtype=jnp.int32)[:, None]
    col_idx = jnp.arange(key_span, dtype=jnp.int32)[None, :]
    distance = reach_rows + row_idx - col_idx
    table_idx = jnp.clip(distance, -MAXREL, MAXREL) + MAXREL
    rel_terms = jnp.take(bias_table, table_idx, axis=1)

    def one_block(block_idx):
        start_row = (block_idx * 128).astype(jnp.int32)
        query_sub = lax.dynamic_slice_in_dim(queries, start_row, 128, 0).reshape(128, HEADS, HEAD).astype(jnp.float32)
        key_sub = lax.dynamic_slice_in_dim(key_pad, start_row, key_span, 0).reshape(key_span, HEADS, HEAD).astype(jnp.float32)
        value_sub = lax.dynamic_slice_in_dim(value_pad, start_row, key_span, 0).reshape(key_span, HEADS, HEAD).astype(jnp.float32)
        scores = jnp.einsum('qhd,khd->hqk', query_sub, key_sub) * HEAD ** (-0.5) + rel_terms
        query_pos = start_row + row_idx
        key_pos = start_row - reach_rows + col_idx
        seg_gap = jnp.floor_divide(query_pos, SEG) - jnp.floor_divide(key_pos, SEG)
        allowed = (key_pos >= 0) & (seg_gap >= 0) & (seg_gap <= LEFT)
        scores = jnp.where(allowed[None], scores, -jnp.inf)
        row_max = lax.optimization_barrier(jnp.max(scores, axis=2, keepdims=True))
        weights_raw = jnp.exp(scores - row_max)
        prob_bf = (weights_raw / lax.optimization_barrier(jnp.sum(weights_raw, axis=2, keepdims=True))).astype(jnp.bfloat16)
        result = jnp.einsum('hqk,khd->qhd', prob_bf.astype(jnp.float32), value_sub)
        return result.astype(jnp.bfloat16).reshape(128, HEADS * HEAD)
    blocks = lax.map(one_block, jnp.arange(sub_count, dtype=jnp.int32))
    return blocks.reshape(queries.shape[0], HEADS * HEAD)

def reference(residual, gains, w_query, w_key, w_value, w_out, rel_bias):
    stream = residual
    for layer_idx in range(LAYERS):
        normed = norm_rows(stream, gains[layer_idx, 0]).astype(jnp.bfloat16)
        queries = jnp.dot(normed, w_query[layer_idx], preferred_element_type=jnp.float32).astype(jnp.bfloat16)
        key_rows = jnp.dot(normed, w_key[layer_idx], preferred_element_type=jnp.float32).astype(jnp.bfloat16)
        value_rows = jnp.dot(normed, w_value[layer_idx], preferred_element_type=jnp.float32).astype(jnp.bfloat16)
        attended = attend_all(queries, key_rows, value_rows, rel_bias[layer_idx])
        branch = jnp.dot(attended, w_out[layer_idx], preferred_element_type=jnp.float32)
        stream = (stream.astype(jnp.float32) + norm_rows(branch, gains[layer_idx, 1])).astype(jnp.bfloat16)
    return stream
```

```python
import functools

import jax
import jax.numpy as jnp
from jax import lax
from jax.experimental import pallas as pl
from jax.experimental.pallas import tpu as pltpu
from jax.sharding import PartitionSpec as P

HEAD = 64
SEG = 64
LEFT = 8
MAXREL = 128
BLOCK = 128
EPS = 1e-06
LOG2E = 1.4426950408889634
NEG = -1e30
SENT = 1
MESH = pl.DeviceIdType.MESH
F32 = jnp.float32
BF16 = jnp.bfloat16


def remote(src, dst, send_sem, recv_sem, where):
    return pltpu.make_async_remote_copy(
        src_ref=src,
        dst_ref=dst,
        send_sem=send_sem,
        recv_sem=recv_sem,
        device_id=where,
        device_id_type=MESH,
    )


def kernel(
    tp,
    sp_count,
    res_ref,
    gains_hbm,
    bias_hbm,
    wq_ref,
    wk_ref,
    wv_ref,
    wo_ref,
    out_ref,
    wbuf,
    gather,
    before,
    kbuf,
    vbuf,
    qbuf,
    branch,
    toeplitz,
    sums,
    gains_ref,
    bias_ref,
    final,
    w_sem,
    io_sem,
    g_send,
    g_recv,
    f_send,
    b_send,
    b_recv,
    bf_send,
    h_send,
    h_recv,
    s_send,
    s_recv,
):
    layers = wbuf.shape[0]
    tokens, cols = res_ref.shape
    width = cols * tp
    chunks = tokens // BLOCK
    pairs = cols // 128
    reach = LEFT * SEG
    blocks = reach // BLOCK
    me = lax.axis_index("tp")
    sp = lax.axis_index("sp")
    core = lax.rem(me, 2)
    sibling = me + 1 - 2 * core
    ychips = tp // 2
    first = sp == 0
    last = sp == sp_count - 1

    weights = (wq_ref, wk_ref, wv_ref, wo_ref)

    def weight_copy(l, k):
        return pltpu.make_async_copy(weights[k].at[l], wbuf.at[l, k], w_sem.at[l, k])

    def rows_of(c):
        return pl.ds(pl.multiple_of(c * BLOCK, BLOCK), BLOCK)

    def res_copy(c):
        return pltpu.make_async_copy(
            res_ref.at[rows_of(c)], gather.at[0, 0, me, rows_of(c)], io_sem.at[c]
        )

    def out_copy(c):
        return pltpu.make_async_copy(final.at[rows_of(c)], out_ref.at[rows_of(c)], io_sem.at[c])

    gains_copy = pltpu.make_async_copy(gains_hbm, gains_ref, io_sem.at[chunks])
    bias_copy = pltpu.make_async_copy(bias_hbm, bias_ref, io_sem.at[chunks + 1])

    for c in reversed(range(chunks)):
        res_copy(c).start()
    bias_copy.start()
    gains_copy.start()
    for k in (1, 2, 0):
        weight_copy(0, k).start()

    barrier = pltpu.get_barrier_semaphore()
    for k in range(1, tp):
        pl.semaphore_signal(
            barrier, inc=1, device_id={"tp": lax.rem(me + k, tp)}, device_id_type=MESH
        )
    for k in (1, sp_count - 1):
        pl.semaphore_signal(
            barrier, inc=1, device_id={"sp": lax.rem(sp + k, sp_count)}, device_id_type=MESH
        )
    pl.semaphore_wait(barrier, tp + 1)

    def block_of(kind, l, c, slot):
        return gather.at[kind, l, slot, rows_of(c)]

    def direct(kind, l, c, peer, source):
        ref = block_of(kind, l, c, source)
        return remote(ref, ref, g_send.at[kind, c, peer], g_recv.at[kind, c, source], {"tp": peer})

    def forward(kind, l, c, source):
        ref = block_of(kind, l, c, source)
        return remote(
            ref, ref, f_send.at[kind, c, source // 2], g_recv.at[kind, c, source], {"tp": sibling}
        )

    def others(base):
        return [lax.rem(base + 2 * k, tp) for k in range(1, ychips)]

    def spread(kind, l, c):
        for peer in others(me):
            direct(kind, l, c, peer, me).start()
        direct(kind, l, c, sibling, me).start()

    def relay(kind, l, c):
        for source in others(me):
            direct(kind, l, c, source, source).wait_recv()
            forward(kind, l, c, source).start()

    def arrive(kind, l, c):
        direct(kind, l, c, sibling, sibling).wait_recv()
        for source in others(sibling):
            direct(kind, l, c, sibling, source).wait_recv()
        for source in others(me):
            forward(kind, l, c, source).wait_send()
            direct(kind, l, c, source, me).wait_send()
        direct(kind, l, c, sibling, me).wait_send()

    def pass_on(l, c, source):
        return remote(
            block_of(0, l, c, source),
            before.at[l, source, rows_of(c - SENT)],
            b_send.at[c - SENT, source // 2],
            b_recv.at[l, c - SENT, source],
            {"sp": lax.rem(sp + 1, sp_count)},
        )

    def pass_across(l, c, source):
        ref = before.at[l, source, rows_of(c - SENT)]
        return remote(
            ref,
            ref,
            bf_send.at[c - SENT, source // 2],
            b_recv.at[l, c - SENT, source],
            {"tp": sibling},
        )

    def relay_stream(l, c):
        relay(0, l, c)

        @pl.when((c >= SENT) & ~last)
        def _():
            for source in others(me):
                pass_on(l, c, source).start()

        @pl.when((l == 0) & (c == chunks - 1) & ~last)
        def _():
            for held in reversed(range(SENT, chunks - 2)):
                pass_on(0, held, me).start()

    def update(l, parts):
        old, branches = parts
        branches = [part.astype(F32) for part in branches]
        total = sum(jnp.sum(part * part, axis=1, keepdims=True) for part in branches)
        inv = lax.rsqrt(total / width + EPS)
        gain = gains_ref[l - 1, 1:2, :]
        return [
            (part.astype(F32) + b * inv * gain[:, j * cols : (j + 1) * cols]).astype(BF16)
            for j, (part, b) in enumerate(zip(old, branches))
        ]

    def relay_before(l, c, sources):
        @pl.when(~first)
        def _():
            for source in sources:
                pass_on(l, c, source).wait_recv()
                pass_across(l, c, source).start()

    def halo(l, c, which):
        if which == 0:
            src, dst = kbuf.at[l, rows_of(c + blocks)], kbuf.at[l, rows_of(c)]
        else:
            src, dst = vbuf.at[l, c + blocks], vbuf.at[l, c]
        return remote(
            src,
            dst,
            h_send.at[c, which],
            h_recv.at[l, c, which],
            {"sp": lax.rem(sp + 1, sp_count)},
        )

    def sum_copy(c, peer, source):
        ref = sums.at[c, source]
        return remote(ref, ref, s_send.at[c, peer], s_recv.at[c, source], {"tp": peer})

    for c in reversed(range(chunks)):
        res_copy(c).wait()
        spread(0, 0, c)
        if c >= max(SENT, chunks - 2):

            @pl.when(~last)
            def _():
                pass_on(0, c, me).start()

    @pl.when(first)
    def _():
        for l in range(layers):
            kbuf[l, :reach] = jnp.zeros((reach, cols), BF16)
            vbuf[l, :blocks] = jnp.zeros((blocks, cols, BLOCK), BF16)

    row = lax.broadcasted_iota(jnp.int32, (BLOCK, BLOCK), 0)
    col = lax.broadcasted_iota(jnp.int32, (BLOCK, BLOCK), 1)
    low = col < HEAD
    late = jnp.where((row >= SEG) & (col < SEG), NEG, 0.0).astype(F32)
    place = lax.broadcasted_iota(jnp.int32, (1, 2 * BLOCK), 1)
    early = jnp.where(lax.rem(place, BLOCK) >= SEG, NEG, 0.0).astype(F32)

    def scaled_and_inv(l, parts):
        parts = [part.astype(F32) for part in parts]
        gain = gains_ref[l, 0:1, :]
        scaled = jnp.concatenate(
            [
                (part * gain[:, j * cols : (j + 1) * cols]).astype(BF16)
                for j, part in enumerate(parts)
            ],
            axis=1,
        )
        total = sum(jnp.sum(part * part, axis=1, keepdims=True) for part in parts)
        return scaled, lax.rsqrt(total / width + EPS)

    def store_keys_values(l, slot, scaled, inv):
        key = jnp.dot(scaled, wbuf[l, 1], preferred_element_type=F32)
        kbuf[l, rows_of(slot)] = (key * inv).astype(BF16)
        value = jnp.dot(scaled, wbuf[l, 2], preferred_element_type=F32)
        vbuf[l, slot] = (value * inv).T.astype(BF16)

    def project(l, c):
        arrive(0, l, c)
        rows = rows_of(c)

        @pl.when(l > 0)
        def _():
            own = ([gather[0, k, j, rows] for j in range(tp)] for k in (0, l))
            for j, part in enumerate(update(l, own)):
                gather[0, 0, j, rows] = part

        scaled, inv = scaled_and_inv(l, [gather[0, 0, j, rows] for j in range(tp)])
        query = jnp.dot(scaled, wbuf[l, 0], preferred_element_type=F32)
        qbuf[rows_of(c)] = (query * (inv * (LOG2E * HEAD**-0.5))).astype(BF16)
        store_keys_values(l, c + blocks, scaled, inv)

        @pl.when((c < SENT) & ~last)
        def _():
            halo(l, c, 0).start()
            halo(l, c, 1).start()

    def project_before(l, c):
        @pl.when(~first)
        def _():
            for source in [sibling] + others(sibling):
                pass_across(l, c, source).wait_recv()
            for source in [me] + others(me):
                pass_across(l, c, source).wait_send()
            rows = rows_of(c - SENT)

            @pl.when(l > 0)
            def _():
                halo_parts = ([before[k, j, rows] for j in range(tp)] for k in (0, l))
                for j, part in enumerate(update(l, halo_parts)):
                    before[0, j, rows] = part

            scaled, inv = scaled_and_inv(l, [before[0, j, rows] for j in range(tp)])
            store_keys_values(l, c, scaled, inv)

    def attention(l, c):
        @pl.when((c < SENT) & ~first)
        def _():
            halo(l, c, 0).wait_recv()
            halo(l, c, 1).wait_recv()

        window = pl.ds(pl.multiple_of(c * BLOCK, BLOCK), reach + BLOCK)
        closed = [
            jnp.where(first & (c + i < blocks), NEG, 0.0).astype(F32) for i in range(blocks)
        ]

        def score(pair):
            lanes = slice(pair * 128, (pair + 1) * 128)
            query = qbuf[rows_of(c), lanes]
            zero = jnp.zeros_like(query)
            both = jnp.concatenate(
                [jnp.where(low, query, zero), jnp.where(low, zero, query)], axis=0
            )
            scores = lax.dot_general(
                kbuf[l, window, lanes],
                both,
                (((1,), (1,)), ((), ())),
                preferred_element_type=F32,
            )
            tiles = []
            tops = []
            for i in range(blocks + 1):
                tile = scores[i * BLOCK : (i + 1) * BLOCK]
                if i == 0:
                    tile = jnp.concatenate([tile[:SEG] + early, tile[SEG:]], axis=0)
                if i >= blocks - 1:
                    tile = tile + toeplitz[l, pair, i - blocks + 1]
                top = jnp.max(tile.reshape(BLOCK // 8, 8, 2 * BLOCK), axis=0)
                if i < blocks:
                    top = top + closed[i]
                tiles.append(tile)
                tops.append(top)
            return tiles, jnp.max(functools.reduce(jnp.maximum, tops), axis=0, keepdims=True)

        def mix(pair, tiles, top):
            lanes = slice(pair * 128, (pair + 1) * 128)
            raw = []
            parts = []
            for i in range(blocks + 1):
                tile = jnp.exp2(tiles[i] - (top - closed[i] if i < blocks else top))
                parts.append(jnp.sum(tile.reshape(BLOCK // 8, 8, 2 * BLOCK), axis=0))
                raw.append(tile.astype(BF16))
            total = jnp.sum(functools.reduce(jnp.add, parts), axis=0, keepdims=True)
            values = jnp.concatenate([vbuf[l, c + i, lanes] for i in range(blocks + 1)], axis=1)
            mixed = jnp.dot(values, jnp.concatenate(raw, axis=0), preferred_element_type=F32)
            mixed = mixed * (1.0 / total)
            mixed = jnp.concatenate([mixed[:HEAD, :BLOCK], mixed[HEAD:, BLOCK:]], axis=0)
            gather[1, l, me, rows_of(c), lanes] = mixed.T.astype(BF16)

        held = [score(pair) for pair in range(pairs)]
        for pair in range(pairs):
            mix(pair, *held[pair])
        spread(1, l, c)

    def out_project(l, c):
        arrive(1, l, c)
        whole = jnp.concatenate([gather[1, l, j, rows_of(c)] for j in range(tp)], axis=1)
        value = jnp.dot(whole, wbuf[l, 3], preferred_element_type=F32)

        @pl.when(l < layers - 1)
        def _():
            later = jnp.minimum(l + 1, layers - 1)
            gather[0, later, me, rows_of(c)] = value.astype(BF16)
            spread(0, later, c)

            @pl.when((c >= SENT) & ~last)
            def _():
                pass_on(later, c, me).start()

        @pl.when(l == layers - 1)
        def _():
            branch[rows_of(c)] = value
            square = jnp.sum(value * value, axis=1, keepdims=True)
            sums[c, me] = jnp.broadcast_to(square, (BLOCK, BLOCK)).T[:8]
            for k in range(1, tp):
                sum_copy(c, lax.rem(me + k, tp), me).start()

    def finish(c):
        for k in range(1, tp):
            peer = lax.rem(me + k, tp)
            sum_copy(c, peer, peer).wait_recv()
            sum_copy(c, peer, me).wait_send()
        total = functools.reduce(jnp.add, [sums[c, j] for j in range(tp)])
        inv = lax.rsqrt(total / width + EPS)
        inv = jnp.broadcast_to(inv[0:1], (BLOCK, BLOCK)).T[:, 0:1]
        gain = gains_ref[layers - 1, 1:2, pl.ds(pl.multiple_of(me * cols, 128), cols)]
        new = gather[0, 0, me, rows_of(c)].astype(F32) + branch[rows_of(c)] * inv * gain
        final[rows_of(c)] = new.astype(BF16)
        out_copy(c).start()

    def passed_on(l):
        @pl.when(~last)
        def _():
            for c in range(chunks):
                if c < SENT:
                    halo(l, c, 0).wait_send()
                    halo(l, c, 1).wait_send()
                else:
                    for source in [me] + others(me):
                        pass_on(l, c, source).wait_send()

    def tables(l, carry):
        far = bias_ref[l, :, 2 * MAXREL :]
        near = (bias_ref[l, :, : 2 * MAXREL] - far) * LOG2E
        for h in range(2 * pairs):
            line = jnp.concatenate([jnp.zeros((1, BLOCK), F32), near[h : h + 1]], axis=1)
            line = jnp.broadcast_to(line, (2 * BLOCK, 3 * BLOCK))
            skewed = pltpu.roll(line, 0, 1, stride=1, stride_axis=0)
            at = slice(h % 2 * BLOCK, (h % 2 + 1) * BLOCK)
            toeplitz[l, h // 2, 0, :, at] = skewed[:BLOCK, :BLOCK]
            toeplitz[l, h // 2, 1, :, at] = skewed[BLOCK:, :BLOCK] + late
        return carry

    bias_copy.wait()
    lax.fori_loop(0, layers, tables, 0)
    gains_copy.wait()

    period = 2 * chunks + 1

    def step(g, carry):
        l = jnp.minimum(g // period, layers - 1)
        t = g - l * period

        def stage(lag, count=chunks):
            return (t >= lag) & (t < lag + count)

        def at(lag):
            return chunks - 1 - t + lag

        @pl.when(stage(0))
        def _():
            relay_stream(l, at(0))

        @pl.when(stage(1, chunks - SENT))
        def _():
            relay_before(l, at(1), [me])

        @pl.when(stage(chunks - 1, chunks - SENT))
        def _():
            project_before(l, at(chunks - 1))

        @pl.when(g == 0)
        def _():
            for k in (1, 2, 0):
                weight_copy(0, k).wait()
            weight_copy(0, 3).start()

        @pl.when((t == 0) & (l > 0))
        def _():
            for k in (1, 2, 0, 3):
                weight_copy(l, k).wait()

        @pl.when(stage(0))
        def _():
            project(l, at(0))

        @pl.when((t == 1) & (l < layers - 1))
        def _():
            for k in (1, 2, 0, 3):
                weight_copy(jnp.minimum(l + 1, layers - 1), k).start()

        @pl.when(stage(chunks + 1))
        def _():
            relay(1, l, at(chunks + 1))

        @pl.when(stage(chunks - 1))
        def _():
            attention(l, at(chunks - 1))

        @pl.when(stage(chunks - 2, chunks - SENT))
        def _():
            relay_before(l, at(chunks - 2), others(me))

        @pl.when(g == chunks + 1)
        def _():
            weight_copy(0, 3).wait()

        @pl.when(t == chunks + 1)
        def _():
            passed_on(l)

        @pl.when(stage(chunks + 1))
        def _():
            out_project(l, at(chunks + 1))

        @pl.when(stage(chunks + 3) & (l == layers - 1))
        def _():
            finish(at(chunks + 3))

        return carry

    lax.fori_loop(0, layers * period + 2, step, 0)
    for c in range(chunks):
        out_copy(c).wait()


def on_device(tp, sp_count, residual, gains, w_query, w_key, w_value, w_out, rel_bias):
    tokens, cols = residual.shape
    layers, width, _ = w_query.shape
    chunks = tokens // BLOCK
    reach = LEFT * SEG
    pairs = cols // 128
    ychips = tp // 2
    hbm = pl.BlockSpec(memory_space=pl.ANY)
    dma = pltpu.SemaphoreType.DMA
    return pl.pallas_call(
        functools.partial(kernel, tp, sp_count),
        out_shape=jax.ShapeDtypeStruct((tokens, cols), BF16),
        in_specs=[hbm] * 7,
        out_specs=hbm,
        scratch_shapes=[
            pltpu.VMEM((layers, 4, width, cols), BF16),
            pltpu.VMEM((2, layers, tp, tokens, cols), BF16),
            pltpu.VMEM((layers, tp, tokens - SENT * BLOCK, cols), BF16),
            pltpu.VMEM((layers, reach + tokens, cols), BF16),
            pltpu.VMEM((layers, reach // BLOCK + chunks, cols, BLOCK), BF16),
            pltpu.VMEM((tokens, cols), BF16),
            pltpu.VMEM((tokens, cols), F32),
            pltpu.VMEM((layers, pairs, 2, BLOCK, 2 * BLOCK), F32),
            pltpu.VMEM((chunks, tp, 8, BLOCK), F32),
            pltpu.VMEM(gains.shape, F32),
            pltpu.VMEM(rel_bias.shape, F32),
            pltpu.VMEM((tokens, cols), BF16),
            dma((layers, 4)),
            dma((chunks + 2,)),
            dma((2, chunks, tp)),
            dma((2, chunks, tp)),
            dma((2, chunks, ychips)),
            dma((chunks - SENT, ychips)),
            dma((layers, chunks - SENT, tp)),
            dma((chunks - SENT, ychips)),
            dma((SENT, 2)),
            dma((layers, SENT, 2)),
            dma((chunks, tp)),
            dma((chunks, tp)),
        ],
        compiler_params=pltpu.CompilerParams(
            collective_id=0, has_side_effects=True, vmem_limit_bytes=58 * 2**20
        ),
    )(residual, gains, rel_bias, w_query, w_key, w_value, w_out)


def solution(mesh):
    return jax.shard_map(
        functools.partial(on_device, mesh.shape["tp"], mesh.shape["sp"]),
        mesh=mesh,
        in_specs=(
            P("sp", "tp"),
            P(),
            P(None, None, "tp"),
            P(None, None, "tp"),
            P(None, None, "tp"),
            P(None, None, "tp"),
            P(None, "tp", None),
        ),
        out_specs=P("sp", "tp"),
        check_vma=False,
    )
```

```python
import functools

import jax
import jax.numpy as jnp
from jax import lax
from jax.experimental import pallas as pl
from jax.experimental.pallas import tpu as pltpu
from jax.sharding import PartitionSpec as P

HEAD = 64
SEG = 64
LEFT = 8
MAXREL = 128
BLOCK = 128
EPS = 1e-06
LOG2E = 1.4426950408889634
NEG = -1e30
SENT = 1
MESH = pl.DeviceIdType.MESH
F32 = jnp.float32
BF16 = jnp.bfloat16


def remote(src, dst, send_sem, recv_sem, where):
    return pltpu.make_async_remote_copy(
        src_ref=src,
        dst_ref=dst,
        send_sem=send_sem,
        recv_sem=recv_sem,
        device_id=where,
        device_id_type=MESH,
    )


def kernel(
    tp,
    sp_count,
    res_ref,
    gains_hbm,
    bias_hbm,
    wq_ref,
    wk_ref,
    wv_ref,
    wo_ref,
    out_ref,
    wbuf,
    gather,
    before,
    kbuf,
    vbuf,
    qbuf,
    branch,
    toeplitz,
    sums,
    gains_ref,
    bias_ref,
    final,
    w_sem,
    io_sem,
    g_send,
    g_recv,
    f_send,
    b_send,
    b_recv,
    bf_send,
    h_send,
    h_recv,
    s_send,
    s_recv,
):
    layers = wbuf.shape[0]
    tokens, cols = res_ref.shape
    width = cols * tp
    chunks = tokens // BLOCK
    pairs = cols // 128
    reach = LEFT * SEG
    blocks = reach // BLOCK
    me = lax.axis_index("tp")
    sp = lax.axis_index("sp")
    core = lax.rem(me, 2)
    sibling = me + 1 - 2 * core
    ychips = tp // 2
    first = sp == 0
    last = sp == sp_count - 1

    weights = (wq_ref, wk_ref, wv_ref, wo_ref)

    def weight_copy(l, k):
        return pltpu.make_async_copy(weights[k].at[l], wbuf.at[l, k], w_sem.at[l, k])

    def rows_of(c):
        return pl.ds(pl.multiple_of(c * BLOCK, BLOCK), BLOCK)

    def res_copy(c):
        return pltpu.make_async_copy(
            res_ref.at[rows_of(c)], gather.at[0, 0, me, rows_of(c)], io_sem.at[c]
        )

    def out_copy(c):
        return pltpu.make_async_copy(final.at[rows_of(c)], out_ref.at[rows_of(c)], io_sem.at[c])

    gains_copy = pltpu.make_async_copy(gains_hbm, gains_ref, io_sem.at[chunks])
    bias_copy = pltpu.make_async_copy(bias_hbm, bias_ref, io_sem.at[chunks + 1])

    for c in reversed(range(chunks)):
        res_copy(c).start()
    bias_copy.start()
    gains_copy.start()
    for k in (1, 2, 0):
        weight_copy(0, k).start()

    barrier = pltpu.get_barrier_semaphore()
    for k in range(1, tp):
        pl.semaphore_signal(
            barrier, inc=1, device_id={"tp": lax.rem(me + k, tp)}, device_id_type=MESH
        )

    @pl.when(~first)
    def _():
        pl.semaphore_signal(
            barrier, inc=1, device_id={"sp": jnp.maximum(sp - 1, 0)}, device_id_type=MESH
        )

    pl.semaphore_wait(barrier, jnp.where(last, tp - 1, tp))

    def block_of(kind, l, c, slot):
        return gather.at[kind, l, slot, rows_of(c)]

    def direct(kind, l, c, peer, source):
        ref = block_of(kind, l, c, source)
        return remote(ref, ref, g_send.at[kind, c, peer], g_recv.at[kind, c, source], {"tp": peer})

    def forward(kind, l, c, source):
        ref = block_of(kind, l, c, source)
        return remote(
            ref, ref, f_send.at[kind, c, source // 2], g_recv.at[kind, c, source], {"tp": sibling}
        )

    def others(base):
        return [lax.rem(base + 2 * k, tp) for k in range(1, ychips)]

    def spread(kind, l, c):
        for peer in others(me):
            direct(kind, l, c, peer, me).start()
        direct(kind, l, c, sibling, me).start()

    def relay(kind, l, c):
        for source in others(me):
            direct(kind, l, c, source, source).wait_recv()
            forward(kind, l, c, source).start()

    def arrive(kind, l, c):
        direct(kind, l, c, sibling, sibling).wait_recv()
        for source in others(sibling):
            direct(kind, l, c, sibling, source).wait_recv()
        for source in others(me):
            forward(kind, l, c, source).wait_send()
            direct(kind, l, c, source, me).wait_send()
        direct(kind, l, c, sibling, me).wait_send()

    def pass_on(l, c, source):
        return remote(
            block_of(0, l, c, source),
            before.at[l, source, rows_of(c - SENT)],
            b_send.at[c - SENT, source // 2],
            b_recv.at[l, c - SENT, source],
            {"sp": lax.rem(sp + 1, sp_count)},
        )

    def pass_across(l, c, source):
        ref = before.at[l, source, rows_of(c - SENT)]
        return remote(
            ref,
            ref,
            bf_send.at[c - SENT, source // 2],
            b_recv.at[l, c - SENT, source],
            {"tp": sibling},
        )

    def relay_stream(l, c):
        relay(0, l, c)

        @pl.when((c >= SENT) & ~last)
        def _():
            for source in others(me):
                pass_on(l, c, source).start()

        @pl.when((l == 0) & (c == chunks - 1) & ~last)
        def _():
            for held in reversed(range(SENT, chunks - 2)):
                pass_on(0, held, me).start()

    def update(l, parts):
        old, branches = parts
        branches = [part.astype(F32) for part in branches]
        total = sum(jnp.sum(part * part, axis=1, keepdims=True) for part in branches)
        inv = lax.rsqrt(total / width + EPS)
        gain = gains_ref[l - 1, 1:2, :]
        return [
            (part.astype(F32) + b * inv * gain[:, j * cols : (j + 1) * cols]).astype(BF16)
            for j, (part, b) in enumerate(zip(old, branches))
        ]

    def relay_before(l, c, sources):
        @pl.when(~first)
        def _():
            for source in sources:
                pass_on(l, c, source).wait_recv()
                pass_across(l, c, source).start()

    def halo(l, c, which):
        if which == 0:
            src, dst = kbuf.at[l, rows_of(c + blocks)], kbuf.at[l, rows_of(c)]
        else:
            src, dst = vbuf.at[l, c + blocks], vbuf.at[l, c]
        return remote(
            src,
            dst,
            h_send.at[c, which],
            h_recv.at[l, c, which],
            {"sp": lax.rem(sp + 1, sp_count)},
        )

    def sum_copy(c, peer, source):
        ref = sums.at[c, source]
        return remote(ref, ref, s_send.at[c, peer], s_recv.at[c, source], {"tp": peer})

    for c in reversed(range(chunks)):
        res_copy(c).wait()
        spread(0, 0, c)
        if c >= max(SENT, chunks - 2):

            @pl.when(~last)
            def _():
                pass_on(0, c, me).start()

    @pl.when(first)
    def _():
        for l in range(layers):
            kbuf[l, :reach] = jnp.zeros((reach, cols), BF16)
            vbuf[l, :blocks] = jnp.zeros((blocks, cols, BLOCK), BF16)

    row = lax.broadcasted_iota(jnp.int32, (BLOCK, BLOCK), 0)
    col = lax.broadcasted_iota(jnp.int32, (BLOCK, BLOCK), 1)
    low = col < HEAD
    late = jnp.where((row >= SEG) & (col < SEG), NEG, 0.0).astype(F32)
    place = lax.broadcasted_iota(jnp.int32, (1, 2 * BLOCK), 1)
    early = jnp.where(lax.rem(place, BLOCK) >= SEG, NEG, 0.0).astype(F32)

    def scaled_and_inv(l, parts):
        parts = [part.astype(F32) for part in parts]
        gain = gains_ref[l, 0:1, :]
        scaled = jnp.concatenate(
            [
                (part * gain[:, j * cols : (j + 1) * cols]).astype(BF16)
                for j, part in enumerate(parts)
            ],
            axis=1,
        )
        total = sum(jnp.sum(part * part, axis=1, keepdims=True) for part in parts)
        return scaled, lax.rsqrt(total / width + EPS)

    def store_keys_values(l, slot, scaled, inv):
        key = jnp.dot(scaled, wbuf[l, 1], preferred_element_type=F32)
        kbuf[l, rows_of(slot)] = (key * inv).astype(BF16)
        value = jnp.dot(scaled, wbuf[l, 2], preferred_element_type=F32)
        vbuf[l, slot] = (value * inv).T.astype(BF16)

    def project(l, c):
        arrive(0, l, c)
        rows = rows_of(c)

        @pl.when(l > 0)
        def _():
            own = ([gather[0, k, j, rows] for j in range(tp)] for k in (0, l))
            for j, part in enumerate(update(l, own)):
                gather[0, 0, j, rows] = part

        scaled, inv = scaled_and_inv(l, [gather[0, 0, j, rows] for j in range(tp)])
        query = jnp.dot(scaled, wbuf[l, 0], preferred_element_type=F32)
        qbuf[rows_of(c)] = (query * (inv * (LOG2E * HEAD**-0.5))).astype(BF16)
        store_keys_values(l, c + blocks, scaled, inv)

        @pl.when((c < SENT) & ~last)
        def _():
            halo(l, c, 0).start()
            halo(l, c, 1).start()

    def project_before(l, c):
        @pl.when(~first)
        def _():
            for source in [sibling] + others(sibling):
                pass_across(l, c, source).wait_recv()
            for source in [me] + others(me):
                pass_across(l, c, source).wait_send()
            rows = rows_of(c - SENT)

            @pl.when(l > 0)
            def _():
                halo_parts = ([before[k, j, rows] for j in range(tp)] for k in (0, l))
                for j, part in enumerate(update(l, halo_parts)):
                    before[0, j, rows] = part

            scaled, inv = scaled_and_inv(l, [before[0, j, rows] for j in range(tp)])
            store_keys_values(l, c, scaled, inv)

    def attention(l, c):
        @pl.when((c < SENT) & ~first)
        def _():
            halo(l, c, 0).wait_recv()
            halo(l, c, 1).wait_recv()

        window = pl.ds(pl.multiple_of(c * BLOCK, BLOCK), reach + BLOCK)
        closed = [
            jnp.where(first & (c + i < blocks), NEG, 0.0).astype(F32) for i in range(blocks)
        ]

        def score(pair):
            lanes = slice(pair * 128, (pair + 1) * 128)
            query = qbuf[rows_of(c), lanes]
            zero = jnp.zeros_like(query)
            both = jnp.concatenate(
                [jnp.where(low, query, zero), jnp.where(low, zero, query)], axis=0
            )
            scores = lax.dot_general(
                kbuf[l, window, lanes],
                both,
                (((1,), (1,)), ((), ())),
                preferred_element_type=F32,
            )
            tiles = []
            tops = []
            for i in range(blocks + 1):
                tile = scores[i * BLOCK : (i + 1) * BLOCK]
                if i == 0:
                    tile = jnp.concatenate([tile[:SEG] + early, tile[SEG:]], axis=0)
                if i >= blocks - 1:
                    tile = tile + toeplitz[l, pair, i - blocks + 1]
                top = jnp.max(tile.reshape(BLOCK // 8, 8, 2 * BLOCK), axis=0)
                if i < blocks:
                    top = top + closed[i]
                tiles.append(tile)
                tops.append(top)
            return tiles, jnp.max(functools.reduce(jnp.maximum, tops), axis=0, keepdims=True)

        def mix(pair, tiles, top):
            lanes = slice(pair * 128, (pair + 1) * 128)
            raw = []
            parts = []
            for i in range(blocks + 1):
                tile = jnp.exp2(tiles[i] - (top - closed[i] if i < blocks else top))
                parts.append(jnp.sum(tile.reshape(BLOCK // 8, 8, 2 * BLOCK), axis=0))
                raw.append(tile.astype(BF16))
            total = jnp.sum(functools.reduce(jnp.add, parts), axis=0, keepdims=True)
            values = jnp.concatenate([vbuf[l, c + i, lanes] for i in range(blocks + 1)], axis=1)
            mixed = jnp.dot(values, jnp.concatenate(raw, axis=0), preferred_element_type=F32)
            mixed = mixed * (1.0 / total)
            mixed = jnp.concatenate([mixed[:HEAD, :BLOCK], mixed[HEAD:, BLOCK:]], axis=0)
            gather[1, l, me, rows_of(c), lanes] = mixed.T.astype(BF16)

        held = [score(pair) for pair in range(pairs)]
        for pair in range(pairs):
            mix(pair, *held[pair])
        spread(1, l, c)

    def out_project(l, c):
        arrive(1, l, c)
        whole = jnp.concatenate([gather[1, l, j, rows_of(c)] for j in range(tp)], axis=1)
        value = jnp.dot(whole, wbuf[l, 3], preferred_element_type=F32)

        @pl.when(l < layers - 1)
        def _():
            later = jnp.minimum(l + 1, layers - 1)
            gather[0, later, me, rows_of(c)] = value.astype(BF16)
            spread(0, later, c)

            @pl.when((c >= SENT) & ~last)
            def _():
                pass_on(later, c, me).start()

        @pl.when(l == layers - 1)
        def _():
            branch[rows_of(c)] = value
            square = jnp.sum(value * value, axis=1, keepdims=True)
            sums[c, me] = jnp.broadcast_to(square, (BLOCK, BLOCK)).T[:8]
            for k in range(1, tp):
                sum_copy(c, lax.rem(me + k, tp), me).start()

    def finish(c):
        for k in range(1, tp):
            peer = lax.rem(me + k, tp)
            sum_copy(c, peer, peer).wait_recv()
            sum_copy(c, peer, me).wait_send()
        total = functools.reduce(jnp.add, [sums[c, j] for j in range(tp)])
        inv = lax.rsqrt(total / width + EPS)
        inv = jnp.broadcast_to(inv[0:1], (BLOCK, BLOCK)).T[:, 0:1]
        gain = gains_ref[layers - 1, 1:2, pl.ds(pl.multiple_of(me * cols, 128), cols)]
        new = gather[0, 0, me, rows_of(c)].astype(F32) + branch[rows_of(c)] * inv * gain
        final[rows_of(c)] = new.astype(BF16)
        out_copy(c).start()

    def passed_on(l):
        @pl.when(~last)
        def _():
            for c in range(chunks):
                if c < SENT:
                    halo(l, c, 0).wait_send()
                    halo(l, c, 1).wait_send()
                else:
                    for source in [me] + others(me):
                        pass_on(l, c, source).wait_send()

    def tables(l, carry):
        far = bias_ref[l, :, 2 * MAXREL :]
        near = (bias_ref[l, :, : 2 * MAXREL] - far) * LOG2E
        for h in range(2 * pairs):
            line = jnp.concatenate([jnp.zeros((1, BLOCK), F32), near[h : h + 1]], axis=1)
            line = jnp.broadcast_to(line, (2 * BLOCK, 3 * BLOCK))
            skewed = pltpu.roll(line, 0, 1, stride=1, stride_axis=0)
            at = slice(h % 2 * BLOCK, (h % 2 + 1) * BLOCK)
            toeplitz[l, h // 2, 0, :, at] = skewed[:BLOCK, :BLOCK]
            toeplitz[l, h // 2, 1, :, at] = skewed[BLOCK:, :BLOCK] + late
        return carry

    bias_copy.wait()
    lax.fori_loop(0, layers, tables, 0)
    gains_copy.wait()

    period = 2 * chunks

    def step(g, carry):
        def stage(lag, count=chunks):
            index = g - lag
            l = jnp.clip(index // period, 0, layers - 1)
            t = index - l * period
            return (t >= 0) & (t < count), l, chunks - 1 - t

        def on(lag, count=chunks, extra=True):
            live, l, c = stage(lag, count)
            return lambda run: pl.when(live & extra)(lambda: run(l, c))

        def layer_at(lag):
            return jnp.clip((g - lag) // period, 0, layers - 1)

        def relay_rest(l, c):
            pl.when(c >= SENT)(lambda: relay_before(l, c, others(me)))

        on(0)(relay_stream)
        on(chunks - 2, 1)(relay_rest)
        on(chunks - 1, 1, layer_at(chunks - 1) > 0)(lambda l, c: relay_rest(l, c - 1))
        on(chunks - 1, chunks - SENT)(project_before)

        @pl.when(g == 0)
        def _():
            for k in (1, 2, 0):
                weight_copy(0, k).wait()
            weight_copy(0, 3).start()

        @pl.when((g > 0) & (lax.rem(g, period) == 0) & (g < layers * period))
        def _():
            for k in (1, 2, 0, 3):
                weight_copy(layer_at(0), k).wait()

        on(0)(project)
        on(1, chunks - SENT)(lambda l, c: relay_before(l, c, [me]))

        @pl.when((lax.rem(g, period) == 1) & (g < (layers - 1) * period))
        def _():
            for k in (1, 2, 0, 3):
                weight_copy(jnp.minimum(layer_at(0) + 1, layers - 1), k).start()

        on(chunks + 1)(lambda l, c: relay(1, l, c))
        on(chunks - 1)(attention)
        on(chunks - 1, chunks - SENT - 1)(lambda l, c: relay_rest(l, c - 1 - jnp.minimum(l, 1)))

        @pl.when(g == chunks + 1)
        def _():
            weight_copy(0, 3).wait()

        on(chunks + 1, 1)(lambda l, c: passed_on(l))
        on(chunks + 1)(out_project)
        on(chunks + 3, chunks, layer_at(chunks + 3) == layers - 1)(lambda l, c: finish(c))
        return carry

    lax.fori_loop(0, (layers - 1) * period + 2 * chunks + 3, step, 0)
    for c in range(chunks):
        out_copy(c).wait()


def on_device(tp, sp_count, residual, gains, w_query, w_key, w_value, w_out, rel_bias):
    tokens, cols = residual.shape
    layers, width, _ = w_query.shape
    chunks = tokens // BLOCK
    reach = LEFT * SEG
    pairs = cols // 128
    ychips = tp // 2
    hbm = pl.BlockSpec(memory_space=pl.ANY)
    dma = pltpu.SemaphoreType.DMA
    return pl.pallas_call(
        functools.partial(kernel, tp, sp_count),
        out_shape=jax.ShapeDtypeStruct((tokens, cols), BF16),
        in_specs=[hbm] * 7,
        out_specs=hbm,
        scratch_shapes=[
            pltpu.VMEM((layers, 4, width, cols), BF16),
            pltpu.VMEM((2, layers, tp, tokens, cols), BF16),
            pltpu.VMEM((layers, tp, tokens - SENT * BLOCK, cols), BF16),
            pltpu.VMEM((layers, reach + tokens, cols), BF16),
            pltpu.VMEM((layers, reach // BLOCK + chunks, cols, BLOCK), BF16),
            pltpu.VMEM((tokens, cols), BF16),
            pltpu.VMEM((tokens, cols), F32),
            pltpu.VMEM((layers, pairs, 2, BLOCK, 2 * BLOCK), F32),
            pltpu.VMEM((chunks, tp, 8, BLOCK), F32),
            pltpu.VMEM(gains.shape, F32),
            pltpu.VMEM(rel_bias.shape, F32),
            pltpu.VMEM((tokens, cols), BF16),
            dma((layers, 4)),
            dma((chunks + 2,)),
            dma((2, chunks, tp)),
            dma((2, chunks, tp)),
            dma((2, chunks, ychips)),
            dma((chunks - SENT, ychips)),
            dma((layers, chunks - SENT, tp)),
            dma((chunks - SENT, ychips)),
            dma((SENT, 2)),
            dma((layers, SENT, 2)),
            dma((chunks, tp)),
            dma((chunks, tp)),
        ],
        compiler_params=pltpu.CompilerParams(
            collective_id=0, has_side_effects=True, vmem_limit_bytes=58 * 2**20
        ),
    )(residual, gains, rel_bias, w_query, w_key, w_value, w_out)


def solution(mesh):
    return jax.shard_map(
        functools.partial(on_device, mesh.shape["tp"], mesh.shape["sp"]),
        mesh=mesh,
        in_specs=(
            P("sp", "tp"),
            P(),
            P(None, None, "tp"),
            P(None, None, "tp"),
            P(None, None, "tp"),
            P(None, None, "tp"),
            P(None, "tp", None),
        ),
        out_specs=P("sp", "tp"),
        check_vma=False,
    )
```

```python
import functools

import jax
import jax.numpy as jnp
from jax import lax
from jax.experimental import pallas as pl
from jax.experimental.pallas import tpu as pltpu
from jax.sharding import PartitionSpec as P

HEAD = 64
SEG = 64
LEFT = 8
MAXREL = 128
BLOCK = 128
EPS = 1e-06
LOG2E = 1.4426950408889634
NEG = -1e30
SENT = 1
MESH = pl.DeviceIdType.MESH
F32 = jnp.float32
BF16 = jnp.bfloat16


def remote(src, dst, send_sem, recv_sem, where):
    return pltpu.make_async_remote_copy(
        src_ref=src,
        dst_ref=dst,
        send_sem=send_sem,
        recv_sem=recv_sem,
        device_id=where,
        device_id_type=MESH,
    )


def kernel(
    tp,
    sp_count,
    res_ref,
    gains_hbm,
    bias_hbm,
    wq_ref,
    wk_ref,
    wv_ref,
    wo_ref,
    out_ref,
    wbuf,
    gather,
    before,
    kbuf,
    vbuf,
    qbuf,
    branch,
    toeplitz,
    sums,
    gains_ref,
    bias_ref,
    w_sem,
    io_sem,
    g_send,
    g_recv,
    f_send,
    b_send,
    b_recv,
    bf_send,
    h_send,
    h_recv,
    s_send,
    s_recv,
):
    layers = wbuf.shape[0]
    tokens, cols = res_ref.shape
    width = cols * tp
    chunks = tokens // BLOCK
    pairs = cols // 128
    reach = LEFT * SEG
    blocks = reach // BLOCK
    me = lax.axis_index("tp")
    sp = lax.axis_index("sp")
    core = lax.rem(me, 2)
    sibling = me + 1 - 2 * core
    ychips = tp // 2
    first = sp == 0
    last = sp == sp_count - 1

    weights = (wq_ref, wk_ref, wv_ref, wo_ref)

    def weight_copy(l, k):
        return pltpu.make_async_copy(weights[k].at[l], wbuf.at[l, k], w_sem.at[l, k])

    def rows_of(c):
        return pl.ds(pl.multiple_of(c * BLOCK, BLOCK), BLOCK)

    def res_copy(c):
        return pltpu.make_async_copy(
            res_ref.at[rows_of(c)], gather.at[0, 0, me, rows_of(c)], io_sem.at[c]
        )

    gains_copy = pltpu.make_async_copy(gains_hbm, gains_ref, io_sem.at[chunks])
    bias_copy = pltpu.make_async_copy(bias_hbm, bias_ref, io_sem.at[chunks + 1])

    for c in reversed(range(chunks)):
        res_copy(c).start()
    bias_copy.start()
    gains_copy.start()
    for k in (1, 2, 0):
        weight_copy(0, k).start()

    barrier = pltpu.get_barrier_semaphore()
    for k in range(1, tp):
        pl.semaphore_signal(
            barrier, inc=1, device_id={"tp": lax.rem(me + k, tp)}, device_id_type=MESH
        )

    @pl.when(~first)
    def _():
        pl.semaphore_signal(
            barrier, inc=1, device_id={"sp": jnp.maximum(sp - 1, 0)}, device_id_type=MESH
        )

    pl.semaphore_wait(barrier, jnp.where(last, tp - 1, tp))

    def block_of(kind, l, c, slot, lanes=slice(None)):
        return gather.at[kind, l, slot, rows_of(c), lanes]

    def direct(kind, l, c, peer, source, lanes=slice(None)):
        ref = block_of(kind, l, c, source, lanes)
        way = jnp.where(peer == sibling, ychips - 1, lax.rem(peer // 2 + ychips - me // 2, ychips) - 1)
        return remote(ref, ref, g_send.at[c, way], g_recv.at[kind, c, source], {"tp": peer})

    def forward(kind, l, c, source):
        ref = block_of(kind, l, c, source)
        return remote(
            ref, ref, f_send.at[c, source // 2], g_recv.at[kind, c, source], {"tp": sibling}
        )

    def others(base):
        return [lax.rem(base + 2 * k, tp) for k in range(1, ychips)]

    def spread(kind, l, c, lanes=slice(None)):
        for peer in others(me):
            direct(kind, l, c, peer, me, lanes).start()
        direct(kind, l, c, sibling, me, lanes).start()

    def relay(kind, l, c):
        for source in others(me):
            direct(kind, l, c, source, source).wait_recv()
            forward(kind, l, c, source).start()

    def arrive(kind, l, c):
        direct(kind, l, c, sibling, sibling).wait_recv()
        for source in others(sibling):
            direct(kind, l, c, sibling, source).wait_recv()
        for source in others(me):
            forward(kind, l, c, source).wait_send()
            direct(kind, l, c, source, me).wait_send()
        direct(kind, l, c, sibling, me).wait_send()

    def pass_on(l, c, source):
        return remote(
            block_of(0, l, c, source),
            before.at[l, source, rows_of(c - SENT)],
            b_send.at[c - SENT, source // 2],
            b_recv.at[l, c - SENT, source],
            {"sp": lax.rem(sp + 1, sp_count)},
        )

    def pass_across(l, c, source):
        ref = before.at[l, source, rows_of(c - SENT)]
        return remote(
            ref,
            ref,
            bf_send.at[c - SENT, source // 2],
            b_recv.at[l, c - SENT, source],
            {"tp": sibling},
        )

    def relay_stream(l, c):
        relay(0, l, c)

        @pl.when((c >= SENT) & ~last)
        def _():
            for source in others(me):
                pass_on(l, c, source).start()

        @pl.when((l == 0) & (c == chunks - 2) & ~last)
        def _():
            for held in reversed(range(SENT, chunks - 2)):
                pass_on(0, held, me).start()

    def update(l, parts):
        old, branches = parts
        branches = [part.astype(F32) for part in branches]
        total = sum(jnp.sum(part * part, axis=1, keepdims=True) for part in branches)
        inv = lax.rsqrt(total / width + EPS)
        gain = gains_ref[l - 1, 1:2, :]
        return [
            (part.astype(F32) + b * inv * gain[:, j * cols : (j + 1) * cols]).astype(BF16)
            for j, (part, b) in enumerate(zip(old, branches))
        ]

    def relay_before(l, c, sources):
        @pl.when(~first)
        def _():
            for source in sources:
                pass_on(l, c, source).wait_recv()
                pass_across(l, c, source).start()

    def halo(l, c, which):
        if which == 0:
            src, dst = kbuf.at[l, rows_of(c + blocks)], kbuf.at[l, rows_of(c)]
        else:
            src, dst = vbuf.at[l, c + blocks], vbuf.at[l, c]
        return remote(
            src,
            dst,
            h_send.at[c, which],
            h_recv.at[l, c, which],
            {"sp": lax.rem(sp + 1, sp_count)},
        )

    def sum_copy(c, peer, source):
        ref = sums.at[c, source]
        return remote(ref, ref, s_send.at[c, peer], s_recv.at[c, source], {"tp": peer})

    for c in reversed(range(chunks)):
        res_copy(c).wait()
        spread(0, 0, c)
        if c >= max(SENT, chunks - 2):

            @pl.when(~last)
            def _():
                pass_on(0, c, me).start()

    @pl.when(first)
    def _():
        for l in range(layers):
            kbuf[l, :reach] = jnp.zeros((reach, cols), BF16)
            vbuf[l, :blocks] = jnp.zeros((blocks, cols, BLOCK), BF16)

    row = lax.broadcasted_iota(jnp.int32, (BLOCK, BLOCK), 0)
    col = lax.broadcasted_iota(jnp.int32, (BLOCK, BLOCK), 1)
    low = col < HEAD
    late = jnp.where((row >= SEG) & (col < SEG), NEG, 0.0).astype(F32)
    place = lax.broadcasted_iota(jnp.int32, (1, 2 * BLOCK), 1)
    early = jnp.where(lax.rem(place, BLOCK) >= SEG, NEG, 0.0).astype(F32)

    def scaled_and_inv(l, parts):
        parts = [part.astype(F32) for part in parts]
        gain = gains_ref[l, 0:1, :]
        scaled = jnp.concatenate(
            [
                (part * gain[:, j * cols : (j + 1) * cols]).astype(BF16)
                for j, part in enumerate(parts)
            ],
            axis=1,
        )
        total = sum(jnp.sum(part * part, axis=1, keepdims=True) for part in parts)
        return scaled, lax.rsqrt(total / width + EPS)

    def store_keys_values(l, slot, scaled, inv):
        key = jnp.dot(scaled, wbuf[l, 1], preferred_element_type=F32)
        kbuf[l, rows_of(slot)] = (key * inv).astype(BF16)
        value = jnp.dot(scaled, wbuf[l, 2], preferred_element_type=F32)
        vbuf[l, slot] = (value * inv).T.astype(BF16)

    def project(l, c):
        arrive(0, l, c)
        rows = rows_of(c)

        @pl.when(l > 0)
        def _():
            own = ([gather[0, k, j, rows] for j in range(tp)] for k in (0, l))
            for j, part in enumerate(update(l, own)):
                gather[0, 0, j, rows] = part

        scaled, inv = scaled_and_inv(l, [gather[0, 0, j, rows] for j in range(tp)])
        store_keys_values(l, c + blocks, scaled, inv)

        @pl.when((c < SENT) & ~last)
        def _():
            halo(l, c, 0).start()
            halo(l, c, 1).start()

    def ask(l, c):
        rows = rows_of(c)
        scaled, inv = scaled_and_inv(l, [gather[0, 0, j, rows] for j in range(tp)])
        query = jnp.dot(scaled, wbuf[l, 0], preferred_element_type=F32)
        qbuf[rows] = (query * (inv * (LOG2E * HEAD**-0.5))).astype(BF16)

    def project_before(l, c):
        @pl.when(~first)
        def _():
            for source in [sibling] + others(sibling):
                pass_across(l, c, source).wait_recv()
            for source in [me] + others(me):
                pass_across(l, c, source).wait_send()
            rows = rows_of(c - SENT)

            @pl.when(l > 0)
            def _():
                halo_parts = ([before[k, j, rows] for j in range(tp)] for k in (0, l))
                for j, part in enumerate(update(l, halo_parts)):
                    before[0, j, rows] = part

            scaled, inv = scaled_and_inv(l, [before[0, j, rows] for j in range(tp)])
            store_keys_values(l, c, scaled, inv)

    def attention(l, c):
        @pl.when((c < SENT) & ~first)
        def _():
            halo(l, c, 0).wait_recv()
            halo(l, c, 1).wait_recv()

        window = pl.ds(pl.multiple_of(c * BLOCK, BLOCK), reach + BLOCK)
        closed = [
            jnp.where(first & (c + i < blocks), NEG, 0.0).astype(F32) for i in range(blocks)
        ]

        def score(pair):
            lanes = slice(pair * 128, (pair + 1) * 128)
            query = qbuf[rows_of(c), lanes]
            zero = jnp.zeros_like(query)
            both = jnp.concatenate(
                [jnp.where(low, query, zero), jnp.where(low, zero, query)], axis=0
            )
            scores = lax.dot_general(
                kbuf[l, window, lanes],
                both,
                (((1,), (1,)), ((), ())),
                preferred_element_type=F32,
            )
            tiles = []
            tops = []
            for i in range(blocks + 1):
                tile = scores[i * BLOCK : (i + 1) * BLOCK]
                if i == 0:
                    tile = jnp.concatenate([tile[:SEG] + early, tile[SEG:]], axis=0)
                if i >= blocks - 1:
                    tile = tile + toeplitz[l, pair, i - blocks + 1]
                top = jnp.max(tile.reshape(BLOCK // 8, 8, 2 * BLOCK), axis=0)
                if i < blocks:
                    top = top + closed[i]
                tiles.append(tile)
                tops.append(top)
            return tiles, jnp.max(functools.reduce(jnp.maximum, tops), axis=0, keepdims=True)

        def mix(pair, tiles, top):
            lanes = slice(pair * 128, (pair + 1) * 128)
            raw = []
            parts = []
            for i in range(blocks + 1):
                tile = jnp.exp2(tiles[i] - (top - closed[i] if i < blocks else top))
                parts.append(jnp.sum(tile.reshape(BLOCK // 8, 8, 2 * BLOCK), axis=0))
                raw.append(tile.astype(BF16))
            total = jnp.sum(functools.reduce(jnp.add, parts), axis=0, keepdims=True)
            values = jnp.concatenate([vbuf[l, c + i, lanes] for i in range(blocks + 1)], axis=1)
            mixed = jnp.dot(values, jnp.concatenate(raw, axis=0), preferred_element_type=F32)
            mixed = mixed * (1.0 / total)
            mixed = jnp.concatenate([mixed[:HEAD, :BLOCK], mixed[HEAD:, BLOCK:]], axis=0)
            gather[1, l, me, rows_of(c), lanes] = mixed.T.astype(BF16)

        held = [score(pair) for pair in range(pairs)]
        for pair in range(pairs):
            mix(pair, *held[pair])
            if pair == pairs // 2 - 1:
                spread(1, l, c, slice(0, (pair + 1) * 128))
        spread(1, l, c, slice(pairs // 2 * 128, cols))

    def out_product(l, c):
        arrive(1, l, c)
        whole = jnp.concatenate([gather[1, l, j, rows_of(c)] for j in range(tp)], axis=1)
        return jnp.dot(whole, wbuf[l, 3], preferred_element_type=F32)

    def hand_on(l, c):
        later = jnp.minimum(l + 1, layers - 1)
        gather[0, later, me, rows_of(c)] = out_product(l, c).astype(BF16)
        spread(0, later, c)

        @pl.when((c >= SENT) & ~last)
        def _():
            pass_on(later, c, me).start()

    def out_project(l, c):
        value = out_product(l, c)
        branch[rows_of(c)] = value
        square = jnp.sum(value * value, axis=1, keepdims=True)
        sums[c, me] = jnp.broadcast_to(square, (BLOCK, BLOCK)).T[:8]
        for k in range(1, tp):
            sum_copy(c, lax.rem(me + k, tp), me).start()

    def finish(c):
        for k in range(1, tp):
            peer = lax.rem(me + k, tp)
            sum_copy(c, peer, peer).wait_recv()
            sum_copy(c, peer, me).wait_send()
        total = functools.reduce(jnp.add, [sums[c, j] for j in range(tp)])
        inv = lax.rsqrt(total / width + EPS)
        inv = jnp.broadcast_to(inv[0:1], (BLOCK, BLOCK)).T[:, 0:1]
        gain = gains_ref[layers - 1, 1:2, pl.ds(pl.multiple_of(me * cols, 128), cols)]
        new = gather[0, 0, me, rows_of(c)].astype(F32) + branch[rows_of(c)] * inv * gain
        out_ref[rows_of(c)] = new.astype(BF16)

    def passed_on(l):
        @pl.when(~last)
        def _():
            for c in range(chunks):
                if c < SENT:
                    halo(l, c, 0).wait_send()
                    halo(l, c, 1).wait_send()
                else:
                    for source in [me] + others(me):
                        pass_on(l, c, source).wait_send()

    def tables(l, carry):
        far = bias_ref[l, :, 2 * MAXREL :]
        near = (bias_ref[l, :, : 2 * MAXREL] - far) * LOG2E
        for h in range(2 * pairs):
            line = jnp.concatenate([jnp.zeros((1, BLOCK), F32), near[h : h + 1]], axis=1)
            line = jnp.broadcast_to(line, (2 * BLOCK, 3 * BLOCK))
            skewed = pltpu.roll(line, 0, 1, stride=1, stride_axis=0)
            at = slice(h % 2 * BLOCK, (h % 2 + 1) * BLOCK)
            toeplitz[l, h // 2, 0, :, at] = skewed[:BLOCK, :BLOCK]
            toeplitz[l, h // 2, 1, :, at] = skewed[BLOCK:, :BLOCK] + late
        return carry

    bias_copy.wait()
    lax.fori_loop(0, layers, tables, 0)
    gains_copy.wait()

    def closing(t, carry):
        finish(chunks - 1 - t)
        return carry

    period = 2 * chunks

    def step(g, carry):
        def stage(lag, count=chunks):
            index = g - lag
            l = jnp.clip(index // period, 0, layers - 1)
            t = index - l * period
            return (t >= 0) & (t < count), l, chunks - 1 - t

        def on(lag, count=chunks, extra=True):
            live, l, c = stage(lag, count)
            return lambda run: pl.when(live & extra)(lambda: run(l, c))

        def layer_at(lag):
            return jnp.clip((g - lag) // period, 0, layers - 1)

        def relay_rest(l, c):
            pl.when((c >= SENT) & (c < chunks - 2))(lambda: relay_before(l, c, [me]))
            pl.when(c >= SENT)(lambda: relay_before(l, c, others(me)))

        on(0)(relay_stream)
        on(chunks - 2, 1)(relay_rest)
        on(chunks - 1, chunks - SENT)(project_before)

        @pl.when(g == 0)
        def _():
            for k in (1, 2, 0):
                weight_copy(0, k).wait()
            weight_copy(0, 3).start()

        @pl.when((g > 0) & (lax.rem(g, period) == 0) & (g < layers * period))
        def _():
            for k in (1, 2, 0, 3):
                weight_copy(layer_at(0), k).wait()

        on(1, chunks - 2)(ask)
        on(0)(project)
        on(1, 2)(lambda l, c: relay_before(l, c, [me]))
        on(chunks - 1, 1)(lambda l, c: relay_rest(l, c - 1))

        @pl.when((lax.rem(g, period) == 1) & (g < (layers - 1) * period))
        def _():
            for k in (1, 2, 0, 3):
                weight_copy(jnp.minimum(layer_at(0) + 1, layers - 1), k).start()

        on(chunks + 1, chunks, layer_at(chunks + 1) < layers - 1)(lambda l, c: relay(1, l, c))
        on(chunks + 2, chunks, layer_at(chunks + 2) == layers - 1)(lambda l, c: relay(1, l, c))
        on(chunks - 1)(attention)
        on(chunks, 2)(lambda l, c: ask(l, c - chunks + 2))
        on(chunks - 1, chunks - SENT - 2, layer_at(chunks - 1) > 0)(lambda l, c: relay_rest(l, c - 2))
        on(chunks, chunks - SENT - 2, layer_at(chunks) == 0)(lambda l, c: relay_rest(l, c - 2))

        @pl.when(g == chunks + 1)
        def _():
            weight_copy(0, 3).wait()

        on(chunks + 1, 1)(lambda l, c: passed_on(l))
        on(chunks + 1, chunks, layer_at(chunks + 1) < layers - 1)(hand_on)
        on(chunks + 2, chunks, layer_at(chunks + 2) == layers - 1)(out_project)
        return carry

    lax.fori_loop(0, (layers - 1) * period + 2 * chunks + 2, step, 0)
    lax.fori_loop(0, chunks, closing, 0)


def on_device(tp, sp_count, residual, gains, w_query, w_key, w_value, w_out, rel_bias):
    tokens, cols = residual.shape
    layers, width, _ = w_query.shape
    chunks = tokens // BLOCK
    reach = LEFT * SEG
    pairs = cols // 128
    ychips = tp // 2
    hbm = pl.BlockSpec(memory_space=pl.ANY)
    dma = pltpu.SemaphoreType.DMA
    staged = pl.pallas_call(
        functools.partial(kernel, tp, sp_count),
        out_shape=pltpu.VMEM((tokens, cols), BF16),
        in_specs=[hbm] * 7,
        out_specs=pl.BlockSpec(memory_space=pltpu.VMEM),
        scratch_shapes=[
            pltpu.VMEM((layers, 4, width, cols), BF16),
            pltpu.VMEM((2, layers, tp, tokens, cols), BF16),
            pltpu.VMEM((layers, tp, tokens - SENT * BLOCK, cols), BF16),
            pltpu.VMEM((layers, reach + tokens, cols), BF16),
            pltpu.VMEM((layers, reach // BLOCK + chunks, cols, BLOCK), BF16),
            pltpu.VMEM((tokens, cols), BF16),
            pltpu.VMEM((tokens, cols), F32),
            pltpu.VMEM((layers, pairs, 2, BLOCK, 2 * BLOCK), F32),
            pltpu.VMEM((chunks, tp, 8, BLOCK), F32),
            pltpu.VMEM(gains.shape, F32),
            pltpu.VMEM(rel_bias.shape, F32),
            dma((layers, 4)),
            dma((chunks + 2,)),
            dma((chunks, ychips)),
            dma((2, chunks, tp)),
            dma((chunks, ychips)),
            dma((chunks - SENT, ychips)),
            dma((layers, chunks - SENT, tp)),
            dma((chunks - SENT, ychips)),
            dma((SENT, 2)),
            dma((layers, SENT, 2)),
            dma((chunks, tp)),
            dma((chunks, tp)),
        ],
        compiler_params=pltpu.CompilerParams(
            collective_id=0, has_side_effects=True, vmem_limit_bytes=58 * 2**20
        ),
    )(residual, gains, rel_bias, w_query, w_key, w_value, w_out)
    return staged


def solution(mesh):
    return jax.shard_map(
        functools.partial(on_device, mesh.shape["tp"], mesh.shape["sp"]),
        mesh=mesh,
        in_specs=(
            P("sp", "tp"),
            P(),
            P(None, None, "tp"),
            P(None, None, "tp"),
            P(None, None, "tp"),
            P(None, None, "tp"),
            P(None, "tp", None),
        ),
        out_specs=P("sp", "tp"),
        check_vma=False,
    )
```

```python
import functools

import jax
import jax.numpy as jnp
from jax import lax
from jax.experimental import pallas as pl
from jax.experimental.pallas import tpu as pltpu
from jax.sharding import PartitionSpec as P

HEAD = 64
SEG = 64
LEFT = 8
MAXREL = 128
BLOCK = 128
EPS = 1e-06
LOG2E = 1.4426950408889634
NEG = -1e30
SENT = 1
MESH = pl.DeviceIdType.MESH
F32 = jnp.float32
BF16 = jnp.bfloat16


def remote(src, dst, send_sem, recv_sem, where):
    return pltpu.make_async_remote_copy(
        src_ref=src,
        dst_ref=dst,
        send_sem=send_sem,
        recv_sem=recv_sem,
        device_id=where,
        device_id_type=MESH,
    )


def kernel(
    tp,
    sp_count,
    res_ref,
    gains_hbm,
    bias_hbm,
    wq_ref,
    wk_ref,
    wv_ref,
    wo_ref,
    out_ref,
    wbuf,
    gather,
    before,
    kbuf,
    vbuf,
    qbuf,
    branch,
    toeplitz,
    sums,
    gains_ref,
    bias_ref,
    w_sem,
    io_sem,
    g_send,
    g_recv,
    f_send,
    b_send,
    b_recv,
    bf_send,
    h_send,
    h_recv,
):
    layers = wbuf.shape[0]
    tokens, cols = res_ref.shape
    width = cols * tp
    chunks = tokens // BLOCK
    pairs = cols // 128
    reach = LEFT * SEG
    blocks = reach // BLOCK
    me = lax.axis_index("tp")
    sp = lax.axis_index("sp")
    core = lax.rem(me, 2)
    sibling = me + 1 - 2 * core
    ychips = tp // 2
    first = sp == 0
    last = sp == sp_count - 1

    weights = (wq_ref, wk_ref, wv_ref, wo_ref)

    def weight_copy(l, k):
        return pltpu.make_async_copy(weights[k].at[l], wbuf.at[l, k], w_sem.at[l, k])

    def rows_of(c):
        return pl.ds(pl.multiple_of(c * BLOCK, BLOCK), BLOCK)

    def res_copy(c):
        return pltpu.make_async_copy(
            res_ref.at[rows_of(c)], gather.at[0, 0, me, rows_of(c)], io_sem.at[c]
        )

    gains_copy = pltpu.make_async_copy(gains_hbm, gains_ref, io_sem.at[chunks])
    bias_copy = pltpu.make_async_copy(bias_hbm, bias_ref, io_sem.at[chunks + 1])

    for c in reversed(range(chunks)):
        res_copy(c).start()
    bias_copy.start()
    gains_copy.start()
    for k in (1, 2, 0):
        weight_copy(0, k).start()

    barrier = pltpu.get_barrier_semaphore()
    for k in range(1, tp):
        pl.semaphore_signal(
            barrier, inc=1, device_id={"tp": lax.rem(me + k, tp)}, device_id_type=MESH
        )

    @pl.when(~first)
    def _():
        pl.semaphore_signal(
            barrier, inc=1, device_id={"sp": jnp.maximum(sp - 1, 0)}, device_id_type=MESH
        )

    pl.semaphore_wait(barrier, jnp.where(last, tp - 1, tp))

    def block_of(kind, l, c, slot, lanes=slice(None)):
        return gather.at[kind, l, slot, rows_of(c), lanes]

    def direct(kind, l, c, peer, source, lanes=slice(None)):
        ref = block_of(kind, l, c, source, lanes)
        way = jnp.where(peer == sibling, ychips - 1, lax.rem(peer // 2 + ychips - me // 2, ychips) - 1)
        return remote(ref, ref, g_send.at[c, way], g_recv.at[kind, c, source], {"tp": peer})

    def forward(kind, l, c, source):
        ref = block_of(kind, l, c, source)
        return remote(
            ref, ref, f_send.at[c, source // 2], g_recv.at[kind, c, source], {"tp": sibling}
        )

    def others(base):
        return [lax.rem(base + 2 * k, tp) for k in range(1, ychips)]

    def spread(kind, l, c, lanes=slice(None)):
        for peer in others(me):
            direct(kind, l, c, peer, me, lanes).start()
        direct(kind, l, c, sibling, me, lanes).start()

    def relay(kind, l, c):
        for source in others(me):
            direct(kind, l, c, source, source).wait_recv()
            forward(kind, l, c, source).start()

    def arrive(kind, l, c):
        direct(kind, l, c, sibling, sibling).wait_recv()
        for source in others(sibling):
            direct(kind, l, c, sibling, source).wait_recv()
        for source in others(me):
            forward(kind, l, c, source).wait_send()
            direct(kind, l, c, source, me).wait_send()
        direct(kind, l, c, sibling, me).wait_send()

    def pass_on(l, c, source):
        return remote(
            block_of(0, l, c, source),
            before.at[l, source, rows_of(c - SENT)],
            b_send.at[c - SENT, source // 2],
            b_recv.at[l, c - SENT, source],
            {"sp": lax.rem(sp + 1, sp_count)},
        )

    def pass_across(l, c, source):
        ref = before.at[l, source, rows_of(c - SENT)]
        return remote(
            ref,
            ref,
            bf_send.at[c - SENT, source // 2],
            b_recv.at[l, c - SENT, source],
            {"tp": sibling},
        )

    def relay_stream(l, c):
        relay(0, l, c)

        @pl.when((c >= SENT) & ~last)
        def _():
            for source in others(me):
                pass_on(l, c, source).start()

        @pl.when((c == jnp.where(l == 0, chunks - 2, chunks - 1)) & ~last)
        def _():
            for held in reversed(range(SENT, chunks - 2)):
                pass_on(l, held, me).start()

    def update(l, parts):
        old, branches = parts
        branches = [part.astype(F32) for part in branches]
        total = sum(jnp.sum(part * part, axis=1, keepdims=True) for part in branches)
        inv = lax.rsqrt(total / width + EPS)
        gain = gains_ref[l - 1, 1:2, :]
        return [
            (part.astype(F32) + b * inv * gain[:, j * cols : (j + 1) * cols]).astype(BF16)
            for j, (part, b) in enumerate(zip(old, branches))
        ]

    def relay_before(l, c, sources):
        @pl.when(~first)
        def _():
            for source in sources:
                pass_on(l, c, source).wait_recv()
                pass_across(l, c, source).start()

    def halo(l, c, which):
        if which == 0:
            src, dst = kbuf.at[l, rows_of(c + blocks)], kbuf.at[l, rows_of(c)]
        else:
            src, dst = vbuf.at[l, c + blocks], vbuf.at[l, c]
        return remote(
            src,
            dst,
            h_send.at[c, which],
            h_recv.at[l, c, which],
            {"sp": lax.rem(sp + 1, sp_count)},
        )

    def sum_copies(c):
        pairs_of = [(peer, g_send.at[c, k]) for k, peer in enumerate(others(me))]
        pairs_of.append((sibling, g_send.at[c, ychips - 1]))
        pairs_of += [(peer, f_send.at[c, k]) for k, peer in enumerate(others(sibling))]

        def copy(peer, source, sem):
            ref = sums.at[c, source]
            return remote(ref, ref, sem, g_recv.at[0, c, source], {"tp": peer})

        return [(copy(peer, me, sem), copy(peer, peer, sem)) for peer, sem in pairs_of]

    for c in reversed(range(chunks)):
        res_copy(c).wait()
        spread(0, 0, c)
        if c >= max(SENT, chunks - 2):

            @pl.when(~last)
            def _():
                pass_on(0, c, me).start()

    @pl.when(first)
    def _():
        for l in range(layers):
            kbuf[l, :reach] = jnp.zeros((reach, cols), BF16)
            vbuf[l, :blocks] = jnp.zeros((blocks, cols, BLOCK), BF16)

    row = lax.broadcasted_iota(jnp.int32, (BLOCK, BLOCK), 0)
    col = lax.broadcasted_iota(jnp.int32, (BLOCK, BLOCK), 1)
    low = col < HEAD
    late = jnp.where((row >= SEG) & (col < SEG), NEG, 0.0).astype(F32)
    place = lax.broadcasted_iota(jnp.int32, (1, 2 * BLOCK), 1)
    early = jnp.where(lax.rem(place, BLOCK) >= SEG, NEG, 0.0).astype(F32)

    def scaled_and_inv(l, parts):
        parts = [part.astype(F32) for part in parts]
        gain = gains_ref[l, 0:1, :]
        scaled = jnp.concatenate(
            [
                (part * gain[:, j * cols : (j + 1) * cols]).astype(BF16)
                for j, part in enumerate(parts)
            ],
            axis=1,
        )
        total = sum(jnp.sum(part * part, axis=1, keepdims=True) for part in parts)
        return scaled, lax.rsqrt(total / width + EPS)

    def store_keys_values(l, slot, scaled, inv):
        key = jnp.dot(scaled, wbuf[l, 1], preferred_element_type=F32)
        kbuf[l, rows_of(slot)] = (key * inv).astype(BF16)
        value = jnp.dot(scaled, wbuf[l, 2], preferred_element_type=F32)
        vbuf[l, slot] = (value * inv).T.astype(BF16)

    def project(l, c):
        arrive(0, l, c)
        rows = rows_of(c)

        @pl.when(l > 0)
        def _():
            own = ([gather[0, k, j, rows] for j in range(tp)] for k in (0, l))
            for j, part in enumerate(update(l, own)):
                gather[0, 0, j, rows] = part

        scaled, inv = scaled_and_inv(l, [gather[0, 0, j, rows] for j in range(tp)])
        store_keys_values(l, c + blocks, scaled, inv)

        @pl.when((c < SENT) & ~last)
        def _():
            halo(l, c, 0).start()
            halo(l, c, 1).start()

    def ask(l, c):
        rows = rows_of(c)
        scaled, inv = scaled_and_inv(l, [gather[0, 0, j, rows] for j in range(tp)])
        query = jnp.dot(scaled, wbuf[l, 0], preferred_element_type=F32)
        qbuf[rows] = (query * (inv * (LOG2E * HEAD**-0.5))).astype(BF16)

    def project_before(l, c):
        @pl.when(~first)
        def _():
            for source in [sibling] + others(sibling):
                pass_across(l, c, source).wait_recv()
            for source in [me] + others(me):
                pass_across(l, c, source).wait_send()
            rows = rows_of(c - SENT)

            @pl.when(l > 0)
            def _():
                halo_parts = ([before[k, j, rows] for j in range(tp)] for k in (0, l))
                for j, part in enumerate(update(l, halo_parts)):
                    before[0, j, rows] = part

            scaled, inv = scaled_and_inv(l, [before[0, j, rows] for j in range(tp)])
            store_keys_values(l, c, scaled, inv)

    def attention(l, c):
        @pl.when((c < SENT) & ~first)
        def _():
            halo(l, c, 0).wait_recv()
            halo(l, c, 1).wait_recv()

        window = pl.ds(pl.multiple_of(c * BLOCK, BLOCK), reach + BLOCK)
        closed = [
            jnp.where(first & (c + i < blocks), NEG, 0.0).astype(F32) for i in range(blocks)
        ]

        def score(pair):
            lanes = slice(pair * 128, (pair + 1) * 128)
            query = qbuf[rows_of(c), lanes]
            zero = jnp.zeros_like(query)
            both = jnp.concatenate(
                [jnp.where(low, query, zero), jnp.where(low, zero, query)], axis=0
            )
            scores = lax.dot_general(
                kbuf[l, window, lanes],
                both,
                (((1,), (1,)), ((), ())),
                preferred_element_type=F32,
            )
            tiles = []
            tops = []
            for i in range(blocks + 1):
                tile = scores[i * BLOCK : (i + 1) * BLOCK]
                if i == 0:
                    tile = jnp.concatenate([tile[:SEG] + early, tile[SEG:]], axis=0)
                if i >= blocks - 1:
                    tile = tile + toeplitz[l, pair, i - blocks + 1]
                top = jnp.max(tile.reshape(BLOCK // 8, 8, 2 * BLOCK), axis=0)
                if i < blocks:
                    top = top + closed[i]
                tiles.append(tile)
                tops.append(top)
            return tiles, jnp.max(functools.reduce(jnp.maximum, tops), axis=0, keepdims=True)

        def mix(pair, tiles, top):
            lanes = slice(pair * 128, (pair + 1) * 128)
            raw = []
            parts = []
            for i in range(blocks + 1):
                tile = jnp.exp2(tiles[i] - (top - closed[i] if i < blocks else top))
                parts.append(jnp.sum(tile.reshape(BLOCK // 8, 8, 2 * BLOCK), axis=0))
                raw.append(tile.astype(BF16))
            total = jnp.sum(functools.reduce(jnp.add, parts), axis=0, keepdims=True)
            values = jnp.concatenate([vbuf[l, c + i, lanes] for i in range(blocks + 1)], axis=1)
            mixed = jnp.dot(values, jnp.concatenate(raw, axis=0), preferred_element_type=F32)
            mixed = mixed * (1.0 / total)
            mixed = jnp.concatenate([mixed[:HEAD, :BLOCK], mixed[HEAD:, BLOCK:]], axis=0)
            gather[1, l, me, rows_of(c), lanes] = mixed.T.astype(BF16)

        held = [score(pair) for pair in range(pairs)]
        for pair in range(pairs):
            mix(pair, *held[pair])
            if pair == pairs // 2 - 1:
                spread(1, l, c, slice(0, (pair + 1) * 128))
        spread(1, l, c, slice(pairs // 2 * 128, cols))

    def out_product(l, c):
        arrive(1, l, c)
        whole = jnp.concatenate([gather[1, l, j, rows_of(c)] for j in range(tp)], axis=1)
        return jnp.dot(whole, wbuf[l, 3], preferred_element_type=F32)

    def hand_on(l, c):
        later = jnp.minimum(l + 1, layers - 1)
        gather[0, later, me, rows_of(c)] = out_product(l, c).astype(BF16)
        spread(0, later, c)

        @pl.when((c >= max(SENT, chunks - 2)) & ~last)
        def _():
            pass_on(later, c, me).start()

    def out_project(l, c):
        value = out_product(l, c)
        branch[rows_of(c)] = value
        square = jnp.sum(value * value, axis=1, keepdims=True)
        sums[c, me] = jnp.broadcast_to(square, (BLOCK, BLOCK)).T[:8]
        for mine, _ in sum_copies(c):
            mine.start()

    def finish(c):
        for mine, theirs in sum_copies(c):
            theirs.wait_recv()
            mine.wait_send()
        total = functools.reduce(jnp.add, [sums[c, j] for j in range(tp)])
        inv = lax.rsqrt(total / width + EPS)
        inv = jnp.broadcast_to(inv[0:1], (BLOCK, BLOCK)).T[:, 0:1]
        gain = gains_ref[layers - 1, 1:2, pl.ds(pl.multiple_of(me * cols, 128), cols)]
        new = gather[0, 0, me, rows_of(c)].astype(F32) + branch[rows_of(c)] * inv * gain
        out_ref[rows_of(c)] = new.astype(BF16)

    def passed_on(l):
        @pl.when(~last)
        def _():
            for c in range(chunks):
                if c < SENT:
                    halo(l, c, 0).wait_send()
                    halo(l, c, 1).wait_send()
                else:
                    for source in [me] + others(me):
                        pass_on(l, c, source).wait_send()

    def tables(l, carry):
        far = bias_ref[l, :, 2 * MAXREL :]
        near = (bias_ref[l, :, : 2 * MAXREL] - far) * LOG2E
        for h in range(2 * pairs):
            line = jnp.concatenate([jnp.zeros((1, BLOCK), F32), near[h : h + 1]], axis=1)
            line = jnp.broadcast_to(line, (2 * BLOCK, 3 * BLOCK))
            skewed = pltpu.roll(line, 0, 1, stride=1, stride_axis=0)
            at = slice(h % 2 * BLOCK, (h % 2 + 1) * BLOCK)
            toeplitz[l, h // 2, 0, :, at] = skewed[:BLOCK, :BLOCK]
            toeplitz[l, h // 2, 1, :, at] = skewed[BLOCK:, :BLOCK] + late
        return carry

    bias_copy.wait()
    lax.fori_loop(0, layers, tables, 0)
    gains_copy.wait()

    def closing(t, carry):
        finish(chunks - 1 - t)
        return carry

    period = 2 * chunks

    def step(g, carry):
        def stage(lag, count=chunks):
            index = g - lag
            l = jnp.clip(index // period, 0, layers - 1)
            t = index - l * period
            return (t >= 0) & (t < count), l, chunks - 1 - t

        def on(lag, count=chunks, extra=True):
            live, l, c = stage(lag, count)
            return lambda run: pl.when(live & extra)(lambda: run(l, c))

        def layer_at(lag):
            return jnp.clip((g - lag) // period, 0, layers - 1)

        def relay_rest(l, c):
            pl.when((c >= SENT) & (c < chunks - 2))(lambda: relay_before(l, c, [me]))
            pl.when(c >= SENT)(lambda: relay_before(l, c, others(me)))

        on(0)(relay_stream)
        on(1, 2)(lambda l, c: relay_before(l, c, [me]))
        live, l, c = stage(1, 2)
        pl.when(live & (c == jnp.where(l == 0, chunks - 2, chunks - 1)))(
            lambda: relay_rest(l, chunks - 1)
        )
        before_live, before_l, c = stage(chunks - 2, chunks - SENT + 1)
        u = chunks - 1 - c
        before_c = jnp.where(u == 0, chunks - 1, chunks - u)
        pl.when(before_live & (u != jnp.where(before_l == 0, 0, 1)))(
            lambda: project_before(before_l, before_c)
        )

        @pl.when(g == 0)
        def _():
            for k in (1, 2, 0):
                weight_copy(0, k).wait()
            weight_copy(0, 3).start()

        @pl.when((g > 0) & (lax.rem(g, period) == 0) & (g < layers * period))
        def _():
            for k in (1, 2, 0, 3):
                weight_copy(layer_at(0), k).wait()

        ask_live, ask_l, c = stage(1, 3)
        v = chunks - 1 - c

        @pl.when(ask_live & ((v == 0) | (v == jnp.where(ask_l == 0, 1, 2))))
        def _():
            first_c = chunks - 1 - jnp.minimum(v, 1)

            def one(i, carry):
                ask(ask_l, first_c - i)
                return carry

            lax.fori_loop(0, jnp.where(v == 2, 2, 1), one, 0)

        on(0)(project)
        on(chunks - 1, 1)(lambda l, c: relay_rest(l, c - 1))

        @pl.when((lax.rem(g, period) == 1) & (g < (layers - 1) * period))
        def _():
            for k in (1, 2, 0, 3):
                weight_copy(jnp.minimum(layer_at(0) + 1, layers - 1), k).start()

        on(chunks + 1, chunks, layer_at(chunks + 1) < layers - 1)(lambda l, c: relay(1, l, c))
        on(chunks + 2, chunks, layer_at(chunks + 2) == layers - 1)(lambda l, c: relay(1, l, c))
        on(chunks - 1)(attention)
        rest_live, rest_l, rest_c = stage(chunks, 2)
        pl.when(rest_live & ((rest_l == 0) | (rest_c == chunks - 2)))(
            lambda: ask(rest_l, rest_c - chunks + 2)
        )
        on(chunks - 1, chunks - SENT - 2, layer_at(chunks - 1) > 0)(lambda l, c: relay_rest(l, c - 2))
        on(chunks, chunks - SENT - 2, layer_at(chunks) == 0)(lambda l, c: relay_rest(l, c - 2))

        @pl.when(g == chunks + 1)
        def _():
            weight_copy(0, 3).wait()

        on(chunks + 1, 1)(lambda l, c: passed_on(l))
        on(chunks + 1, chunks, layer_at(chunks + 1) < layers - 1)(hand_on)
        on(chunks + 2, chunks, layer_at(chunks + 2) == layers - 1)(out_project)
        return carry

    lax.fori_loop(0, (layers - 1) * period + 2 * chunks + 2, step, 0)
    lax.fori_loop(0, chunks, closing, 0)


def on_device(tp, sp_count, residual, gains, w_query, w_key, w_value, w_out, rel_bias):
    tokens, cols = residual.shape
    layers, width, _ = w_query.shape
    chunks = tokens // BLOCK
    reach = LEFT * SEG
    pairs = cols // 128
    ychips = tp // 2
    hbm = pl.BlockSpec(memory_space=pl.ANY)
    dma = pltpu.SemaphoreType.DMA
    staged = pl.pallas_call(
        functools.partial(kernel, tp, sp_count),
        out_shape=pltpu.VMEM((tokens, cols), BF16),
        in_specs=[hbm] * 7,
        out_specs=pl.BlockSpec(memory_space=pltpu.VMEM),
        scratch_shapes=[
            pltpu.VMEM((layers, 4, width, cols), BF16),
            pltpu.VMEM((2, layers, tp, tokens, cols), BF16),
            pltpu.VMEM((layers, tp, tokens - SENT * BLOCK, cols), BF16),
            pltpu.VMEM((layers, reach + tokens, cols), BF16),
            pltpu.VMEM((layers, reach // BLOCK + chunks, cols, BLOCK), BF16),
            pltpu.VMEM((tokens, cols), BF16),
            pltpu.VMEM((tokens, cols), F32),
            pltpu.VMEM((layers, pairs, 2, BLOCK, 2 * BLOCK), F32),
            pltpu.VMEM((chunks, tp, 8, BLOCK), F32),
            pltpu.VMEM(gains.shape, F32),
            pltpu.VMEM(rel_bias.shape, F32),
            dma((layers, 4)),
            dma((chunks + 2,)),
            dma((chunks, ychips)),
            dma((2, chunks, tp)),
            dma((chunks, ychips)),
            dma((chunks - SENT, ychips)),
            dma((layers, chunks - SENT, tp)),
            dma((chunks - SENT, ychips)),
            dma((SENT, 2)),
            dma((layers, SENT, 2)),
        ],
        compiler_params=pltpu.CompilerParams(
            collective_id=0, has_side_effects=True, vmem_limit_bytes=58 * 2**20
        ),
    )(residual, gains, rel_bias, w_query, w_key, w_value, w_out)
    return staged


def solution(mesh):
    return jax.shard_map(
        functools.partial(on_device, mesh.shape["tp"], mesh.shape["sp"]),
        mesh=mesh,
        in_specs=(
            P("sp", "tp"),
            P(),
            P(None, None, "tp"),
            P(None, None, "tp"),
            P(None, None, "tp"),
            P(None, None, "tp"),
            P(None, "tp", None),
        ),
        out_specs=P("sp", "tp"),
        check_vma=False,
    )
```

```python
import functools

import jax
import jax.numpy as jnp
from jax import lax
from jax.experimental import pallas as pl
from jax.experimental.pallas import tpu as pltpu
from jax.sharding import PartitionSpec as P

HEAD = 64
SEG = 64
LEFT = 8
MAXREL = 128
BLOCK = 128
EPS = 1e-06
LOG2E = 1.4426950408889634
NEG = -1e30
SENT = 1
MESH = pl.DeviceIdType.MESH
F32 = jnp.float32
BF16 = jnp.bfloat16


def remote(src, dst, send_sem, recv_sem, where):
    return pltpu.make_async_remote_copy(
        src_ref=src,
        dst_ref=dst,
        send_sem=send_sem,
        recv_sem=recv_sem,
        device_id=where,
        device_id_type=MESH,
    )


def kernel(
    tp,
    sp_count,
    res_ref,
    gains_hbm,
    bias_hbm,
    wq_ref,
    wk_ref,
    wv_ref,
    wo_ref,
    out_ref,
    wbuf,
    gather,
    before,
    kbuf,
    vbuf,
    qbuf,
    branch,
    toeplitz,
    sums,
    gains_ref,
    bias_ref,
    w_sem,
    io_sem,
    g_send,
    g_recv,
    f_send,
    b_send,
    b_recv,
    bf_send,
    h_send,
    h_recv,
):
    layers = wbuf.shape[0]
    tokens, cols = res_ref.shape
    width = cols * tp
    chunks = tokens // BLOCK
    pairs = cols // 128
    reach = LEFT * SEG
    blocks = reach // BLOCK
    me = lax.axis_index("tp")
    sp = lax.axis_index("sp")
    core = lax.rem(me, 2)
    sibling = me + 1 - 2 * core
    ychips = tp // 2
    first = sp == 0
    last = sp == sp_count - 1

    weights = (wq_ref, wk_ref, wv_ref, wo_ref)

    def weight_copy(l, k):
        return pltpu.make_async_copy(weights[k].at[l], wbuf.at[l, k], w_sem.at[l, k])

    def rows_of(c):
        return pl.ds(pl.multiple_of(c * BLOCK, BLOCK), BLOCK)

    def res_copy(c):
        return pltpu.make_async_copy(
            res_ref.at[rows_of(c)], gather.at[0, 0, me, rows_of(c)], io_sem.at[c]
        )

    gains_copy = pltpu.make_async_copy(gains_hbm, gains_ref, io_sem.at[chunks])
    bias_copy = pltpu.make_async_copy(bias_hbm, bias_ref, io_sem.at[chunks + 1])

    for c in reversed(range(chunks)):
        res_copy(c).start()
    bias_copy.start()
    gains_copy.start()
    for k in (1, 2, 0):
        weight_copy(0, k).start()

    barrier = pltpu.get_barrier_semaphore()
    for k in range(1, tp):
        pl.semaphore_signal(
            barrier, inc=1, device_id={"tp": lax.rem(me + k, tp)}, device_id_type=MESH
        )

    @pl.when(~first)
    def _():
        pl.semaphore_signal(
            barrier, inc=1, device_id={"sp": jnp.maximum(sp - 1, 0)}, device_id_type=MESH
        )

    pl.semaphore_wait(barrier, jnp.where(last, tp - 1, tp))

    def block_of(kind, l, c, slot, lanes=slice(None)):
        return gather.at[kind, l, slot, rows_of(c), lanes]

    def direct(kind, l, c, peer, source, lanes=slice(None)):
        ref = block_of(kind, l, c, source, lanes)
        way = jnp.where(peer == sibling, ychips - 1, lax.rem(peer // 2 + ychips - me // 2, ychips) - 1)
        return remote(ref, ref, g_send.at[c, way], g_recv.at[kind, c, source], {"tp": peer})

    def forward(kind, l, c, source):
        ref = block_of(kind, l, c, source)
        return remote(
            ref, ref, f_send.at[c, source // 2], g_recv.at[kind, c, source], {"tp": sibling}
        )

    def others(base):
        return [lax.rem(base + 2 * k, tp) for k in range(1, ychips)]

    def spread(kind, l, c, lanes=slice(None)):
        for peer in others(me):
            direct(kind, l, c, peer, me, lanes).start()
        direct(kind, l, c, sibling, me, lanes).start()

    def relay(kind, l, c):
        for source in others(me):
            direct(kind, l, c, source, source).wait_recv()
            forward(kind, l, c, source).start()

    def arrive(kind, l, c):
        direct(kind, l, c, sibling, sibling).wait_recv()
        for source in others(sibling):
            direct(kind, l, c, sibling, source).wait_recv()
        sent(kind, l, c)

    def sent(kind, l, c):
        for source in others(me):
            forward(kind, l, c, source).wait_send()
            direct(kind, l, c, source, me).wait_send()
        direct(kind, l, c, sibling, me).wait_send()

    def pass_on(l, c, source):
        return remote(
            block_of(0, l, c, source),
            before.at[l, source, rows_of(c - SENT)],
            b_send.at[c - SENT, source // 2],
            b_recv.at[l, c - SENT, source],
            {"sp": lax.rem(sp + 1, sp_count)},
        )

    def pass_across(l, c, source):
        ref = before.at[l, source, rows_of(c - SENT)]
        return remote(
            ref,
            ref,
            bf_send.at[c - SENT, source // 2],
            b_recv.at[l, c - SENT, source],
            {"tp": sibling},
        )

    def relay_stream(l, c):
        relay(0, l, c)

        @pl.when((c >= SENT) & ~last)
        def _():
            for source in others(me):
                pass_on(l, c, source).start()

        @pl.when((c == jnp.where(l == 0, chunks - 2, chunks - 1)) & ~last)
        def _():
            for held in reversed(range(SENT, chunks - 2)):
                pass_on(l, held, me).start()

    def update(l, parts):
        old, branches = parts
        branches = [part.astype(F32) for part in branches]
        total = sum(jnp.sum(part * part, axis=1, keepdims=True) for part in branches)
        inv = lax.rsqrt(total / width + EPS)
        gain = gains_ref[l - 1, 1:2, :]
        return [
            (part.astype(F32) + b * inv * gain[:, j * cols : (j + 1) * cols]).astype(BF16)
            for j, (part, b) in enumerate(zip(old, branches))
        ]

    def relay_before(l, c, sources):
        @pl.when(~first)
        def _():
            for source in sources:
                pass_on(l, c, source).wait_recv()
                pass_across(l, c, source).start()

    def halo(l, c, which):
        if which == 0:
            src, dst = kbuf.at[l, rows_of(c + blocks)], kbuf.at[l, rows_of(c)]
        else:
            src, dst = vbuf.at[l, c + blocks], vbuf.at[l, c]
        return remote(
            src,
            dst,
            h_send.at[c, which],
            h_recv.at[l, c, which],
            {"sp": lax.rem(sp + 1, sp_count)},
        )

    def sum_copies(c):
        pairs_of = [(peer, g_send.at[c, k]) for k, peer in enumerate(others(me))]
        pairs_of.append((sibling, g_send.at[c, ychips - 1]))
        pairs_of += [(peer, f_send.at[c, k]) for k, peer in enumerate(others(sibling))]

        def copy(peer, source, sem):
            ref = sums.at[c, source]
            return remote(ref, ref, sem, g_recv.at[0, c, source], {"tp": peer})

        return [(copy(peer, me, sem), copy(peer, peer, sem)) for peer, sem in pairs_of]

    for c in reversed(range(chunks)):
        res_copy(c).wait()
        spread(0, 0, c)
        if c >= max(SENT, chunks - 2):

            @pl.when(~last)
            def _():
                pass_on(0, c, me).start()

    @pl.when(first)
    def _():
        for l in range(layers):
            kbuf[l, :reach] = jnp.zeros((reach, cols), BF16)
            vbuf[l, :blocks] = jnp.zeros((blocks, cols, BLOCK), BF16)

    row = lax.broadcasted_iota(jnp.int32, (BLOCK, BLOCK), 0)
    col = lax.broadcasted_iota(jnp.int32, (BLOCK, BLOCK), 1)
    low = col < HEAD
    late = jnp.where((row >= SEG) & (col < SEG), NEG, 0.0).astype(F32)
    place = lax.broadcasted_iota(jnp.int32, (1, 2 * BLOCK), 1)
    early = jnp.where(lax.rem(place, BLOCK) >= SEG, NEG, 0.0).astype(F32)

    def scaled_and_inv(l, parts):
        parts = [part.astype(F32) for part in parts]
        gain = gains_ref[l, 0:1, :]
        scaled = jnp.concatenate(
            [
                (part * gain[:, j * cols : (j + 1) * cols]).astype(BF16)
                for j, part in enumerate(parts)
            ],
            axis=1,
        )
        total = sum(jnp.sum(part * part, axis=1, keepdims=True) for part in parts)
        return scaled, lax.rsqrt(total / width + EPS)

    def store_keys_values(l, slot, scaled, inv):
        value = jnp.dot(scaled, wbuf[l, 2], preferred_element_type=F32)
        vbuf[l, slot] = (value * inv).T.astype(BF16)
        key = jnp.dot(scaled, wbuf[l, 1], preferred_element_type=F32)
        kbuf[l, rows_of(slot)] = (key * inv).astype(BF16)

    def project(l, c):
        arrive(0, l, c)
        rows = rows_of(c)

        @pl.when(l > 0)
        def _():
            own = ([gather[0, k, j, rows] for j in range(tp)] for k in (0, l))
            parts = update(l, own)
            for j, part in enumerate(parts):
                gather[0, 0, j, rows] = part
            store_keys_values(l, c + blocks, *scaled_and_inv(l, parts))

        @pl.when(l == 0)
        def _():
            parts = [gather[0, 0, j, rows] for j in range(tp)]
            store_keys_values(l, c + blocks, *scaled_and_inv(l, parts))

        @pl.when((c < SENT) & ~last)
        def _():
            halo(l, c, 0).start()
            halo(l, c, 1).start()

    def ask(l, c):
        rows = rows_of(c)
        scaled, inv = scaled_and_inv(l, [gather[0, 0, j, rows] for j in range(tp)])
        query = jnp.dot(scaled, wbuf[l, 0], preferred_element_type=F32)
        qbuf[rows] = (query * (inv * (LOG2E * HEAD**-0.5))).astype(BF16)

    def project_before(l, c):
        @pl.when(~first)
        def _():
            for source in [sibling] + others(sibling):
                pass_across(l, c, source).wait_recv()
            for source in [me] + others(me):
                pass_across(l, c, source).wait_send()
            rows = rows_of(c - SENT)

            @pl.when(l > 0)
            def _():
                halo_parts = ([before[k, j, rows] for j in range(tp)] for k in (0, l))
                parts = update(l, halo_parts)
                for j, part in enumerate(parts):
                    before[0, j, rows] = part
                store_keys_values(l, c, *scaled_and_inv(l, parts))

            @pl.when(l == 0)
            def _():
                parts = [before[0, j, rows] for j in range(tp)]
                store_keys_values(l, c, *scaled_and_inv(l, parts))

    def attention(l, c):
        @pl.when((c < SENT) & ~first)
        def _():
            halo(l, c, 0).wait_recv()
            halo(l, c, 1).wait_recv()

        window = pl.ds(pl.multiple_of(c * BLOCK, BLOCK), reach + BLOCK)
        closed = [
            jnp.where(first & (c + i < blocks), NEG, 0.0).astype(F32) for i in range(blocks)
        ]

        def score(pair):
            lanes = slice(pair * 128, (pair + 1) * 128)
            query = qbuf[rows_of(c), lanes]
            zero = jnp.zeros_like(query)
            both = jnp.concatenate(
                [jnp.where(low, query, zero), jnp.where(low, zero, query)], axis=0
            )
            scores = lax.dot_general(
                kbuf[l, window, lanes],
                both,
                (((1,), (1,)), ((), ())),
                preferred_element_type=F32,
            )
            tiles = []
            tops = []
            for i in range(blocks + 1):
                tile = scores[i * BLOCK : (i + 1) * BLOCK]
                if i == 0:
                    tile = jnp.concatenate([tile[:SEG] + early, tile[SEG:]], axis=0)
                if i >= blocks - 1:
                    tile = tile + toeplitz[l, pair, i - blocks + 1]
                top = jnp.max(tile.reshape(BLOCK // 8, 8, 2 * BLOCK), axis=0)
                if i < blocks:
                    top = top + closed[i]
                tiles.append(tile)
                tops.append(top)
            return tiles, jnp.max(functools.reduce(jnp.maximum, tops), axis=0, keepdims=True)

        def mix(pair, tiles, top):
            lanes = slice(pair * 128, (pair + 1) * 128)
            raw = []
            parts = []
            for i in range(blocks + 1):
                tile = jnp.exp2(tiles[i] - (top - closed[i] if i < blocks else top))
                parts.append(jnp.sum(tile.reshape(BLOCK // 8, 8, 2 * BLOCK), axis=0))
                raw.append(tile.astype(BF16))
            total = jnp.sum(functools.reduce(jnp.add, parts), axis=0, keepdims=True)
            values = jnp.concatenate([vbuf[l, c + i, lanes] for i in range(blocks + 1)], axis=1)
            mixed = jnp.dot(values, jnp.concatenate(raw, axis=0), preferred_element_type=F32)
            mixed = mixed * (1.0 / total)
            mixed = jnp.concatenate([mixed[:HEAD, :BLOCK], mixed[HEAD:, BLOCK:]], axis=0)
            gather[1, l, me, rows_of(c), lanes] = mixed.T.astype(BF16)

        held = [score(pair) for pair in range(pairs)]
        for pair in range(pairs):
            mix(pair, *held[pair])
            if pair == pairs // 2 - 1:
                spread(1, l, c, slice(0, (pair + 1) * 128))
        spread(1, l, c, slice(pairs // 2 * 128, cols))

    def out_product(l, c):
        arrive(1, l, c)
        whole = jnp.concatenate([gather[1, l, j, rows_of(c)] for j in range(tp)], axis=1)
        return jnp.dot(whole, wbuf[l, 3], preferred_element_type=F32)

    def hand_on(l, c):
        later = jnp.minimum(l + 1, layers - 1)
        gather[0, later, me, rows_of(c)] = out_product(l, c).astype(BF16)
        spread(0, later, c)

        @pl.when((c >= max(SENT, chunks - 2)) & ~last)
        def _():
            pass_on(later, c, me).start()

    def out_project(l, c):
        def product(sources):
            total = None
            for source in sources:
                rows = pl.ds(pl.multiple_of(source * cols, cols), cols)
                part = jnp.dot(
                    gather[1, l, source, rows_of(c)],
                    wbuf[l, 3, rows],
                    preferred_element_type=F32,
                )
                total = part if total is None else total + part
            return total

        direct(1, l, c, sibling, sibling).wait_recv()
        branch[rows_of(c)] = product([me, sibling] + others(me))
        for source in others(sibling):
            direct(1, l, c, sibling, source).wait_recv()
        sent(1, l, c)
        value = branch[rows_of(c)] + product(others(sibling))
        branch[rows_of(c)] = value
        square = jnp.sum(value * value, axis=1, keepdims=True)
        sums[c, me] = jnp.broadcast_to(square, (BLOCK, BLOCK)).T[:8]
        for mine, _ in sum_copies(c):
            mine.start()

    def finish(c):
        for mine, theirs in sum_copies(c):
            theirs.wait_recv()
            mine.wait_send()
        total = functools.reduce(jnp.add, [sums[c, j] for j in range(tp)])
        inv = lax.rsqrt(total / width + EPS)
        inv = jnp.broadcast_to(inv[0:1], (BLOCK, BLOCK)).T[:, 0:1]
        gain = gains_ref[layers - 1, 1:2, pl.ds(pl.multiple_of(me * cols, 128), cols)]
        new = gather[0, 0, me, rows_of(c)].astype(F32) + branch[rows_of(c)] * inv * gain
        out_ref[rows_of(c)] = new.astype(BF16)

    def passed_on(l):
        @pl.when(~last)
        def _():
            for c in range(chunks):
                if c < SENT:
                    halo(l, c, 0).wait_send()
                    halo(l, c, 1).wait_send()
                else:
                    for source in [me] + others(me):
                        pass_on(l, c, source).wait_send()

    def tables(l, carry):
        far = bias_ref[l, :, 2 * MAXREL :]
        near = (bias_ref[l, :, : 2 * MAXREL] - far) * LOG2E
        for h in range(2 * pairs):
            line = jnp.concatenate([jnp.zeros((1, BLOCK), F32), near[h : h + 1]], axis=1)
            line = jnp.broadcast_to(line, (2 * BLOCK, 3 * BLOCK))
            skewed = pltpu.roll(line, 0, 1, stride=1, stride_axis=0)
            at = slice(h % 2 * BLOCK, (h % 2 + 1) * BLOCK)
            toeplitz[l, h // 2, 0, :, at] = skewed[:BLOCK, :BLOCK]
            toeplitz[l, h // 2, 1, :, at] = skewed[BLOCK:, :BLOCK] + late
        return carry

    bias_copy.wait()
    lax.fori_loop(0, layers, tables, 0)
    gains_copy.wait()

    def closing(t, carry):
        finish(chunks - 1 - t)
        return carry

    period = 2 * chunks

    def step(g, carry):
        def stage(lag, count=chunks):
            index = g - lag
            l = jnp.clip(index // period, 0, layers - 1)
            t = index - l * period
            return (t >= 0) & (t < count), l, chunks - 1 - t

        def on(lag, count=chunks, extra=True):
            live, l, c = stage(lag, count)
            return lambda run: pl.when(live & extra)(lambda: run(l, c))

        def layer_at(lag):
            return jnp.clip((g - lag) // period, 0, layers - 1)

        def relay_rest(l, c):
            pl.when((c >= SENT) & (c < chunks - 2))(lambda: relay_before(l, c, [me]))
            pl.when(c >= SENT)(lambda: relay_before(l, c, others(me)))

        on(0)(relay_stream)
        on(1, 2)(lambda l, c: relay_before(l, c, [me]))
        live, l, c = stage(1, 2)
        pl.when(live & (c == jnp.where(l == 0, chunks - 2, chunks - 1)))(
            lambda: relay_rest(l, chunks - 1)
        )
        before_live, before_l, c = stage(chunks - 2, chunks - SENT + 1)
        u = chunks - 1 - c
        before_c = jnp.where(u == 0, chunks - 1, chunks - u)
        pl.when(before_live & (u != jnp.where(before_l == 0, 0, 1)))(
            lambda: project_before(before_l, before_c)
        )

        @pl.when(g == 0)
        def _():
            for k in (1, 2, 0):
                weight_copy(0, k).wait()
            weight_copy(0, 3).start()

        @pl.when((g > 0) & (lax.rem(g, period) == 0) & (g < layers * period))
        def _():
            for k in (1, 2, 0, 3):
                weight_copy(layer_at(0), k).wait()

        ask_live, ask_l, c = stage(1, 3)
        v = chunks - 1 - c

        @pl.when(ask_live & ((v == 0) | (v == jnp.where(ask_l == 0, 1, 2))))
        def _():
            first_c = chunks - 1 - jnp.minimum(v, 1)

            def one(i, carry):
                ask(ask_l, first_c - i)
                return carry

            lax.fori_loop(0, jnp.where(v == 2, 2, 1), one, 0)

        on(0)(project)
        on(chunks - 1, 1)(lambda l, c: relay_rest(l, c - 1))

        @pl.when((lax.rem(g, period) == 1) & (g < (layers - 1) * period))
        def _():
            for k in (1, 2, 0, 3):
                weight_copy(jnp.minimum(layer_at(0) + 1, layers - 1), k).start()

        on(chunks + 1, chunks, layer_at(chunks + 1) < layers - 1)(lambda l, c: relay(1, l, c))
        on(chunks + 2, chunks, layer_at(chunks + 2) == layers - 1)(lambda l, c: relay(1, l, c))
        on(chunks - 1)(attention)
        rest_live, rest_l, rest_c = stage(chunks, 2)
        pl.when(rest_live & ((rest_l == 0) | (rest_c == chunks - 2)))(
            lambda: ask(rest_l, rest_c - chunks + 2)
        )
        on(chunks - 1, chunks - SENT - 2, layer_at(chunks - 1) > 0)(lambda l, c: relay_rest(l, c - 2))
        on(chunks, chunks - SENT - 2, layer_at(chunks) == 0)(lambda l, c: relay_rest(l, c - 2))

        @pl.when(g == chunks + 1)
        def _():
            weight_copy(0, 3).wait()

        on(chunks + 1, 1)(lambda l, c: passed_on(l))
        on(chunks + 1, chunks, layer_at(chunks + 1) < layers - 1)(hand_on)
        on(chunks + 2, chunks, layer_at(chunks + 2) == layers - 1)(out_project)
        return carry

    lax.fori_loop(0, (layers - 1) * period + 2 * chunks + 2, step, 0)
    lax.fori_loop(0, chunks, closing, 0)


def on_device(tp, sp_count, residual, gains, w_query, w_key, w_value, w_out, rel_bias):
    tokens, cols = residual.shape
    layers, width, _ = w_query.shape
    chunks = tokens // BLOCK
    reach = LEFT * SEG
    pairs = cols // 128
    ychips = tp // 2
    hbm = pl.BlockSpec(memory_space=pl.ANY)
    dma = pltpu.SemaphoreType.DMA
    staged = pl.pallas_call(
        functools.partial(kernel, tp, sp_count),
        out_shape=pltpu.VMEM((tokens, cols), BF16),
        in_specs=[hbm] * 7,
        out_specs=pl.BlockSpec(memory_space=pltpu.VMEM),
        scratch_shapes=[
            pltpu.VMEM((layers, 4, width, cols), BF16),
            pltpu.VMEM((2, layers, tp, tokens, cols), BF16),
            pltpu.VMEM((layers, tp, tokens - SENT * BLOCK, cols), BF16),
            pltpu.VMEM((layers, reach + tokens, cols), BF16),
            pltpu.VMEM((layers, reach // BLOCK + chunks, cols, BLOCK), BF16),
            pltpu.VMEM((tokens, cols), BF16),
            pltpu.VMEM((tokens, cols), F32),
            pltpu.VMEM((layers, pairs, 2, BLOCK, 2 * BLOCK), F32),
            pltpu.VMEM((chunks, tp, 8, BLOCK), F32),
            pltpu.VMEM(gains.shape, F32),
            pltpu.VMEM(rel_bias.shape, F32),
            dma((layers, 4)),
            dma((chunks + 2,)),
            dma((chunks, ychips)),
            dma((2, chunks, tp)),
            dma((chunks, ychips)),
            dma((chunks - SENT, ychips)),
            dma((layers, chunks - SENT, tp)),
            dma((chunks - SENT, ychips)),
            dma((SENT, 2)),
            dma((layers, SENT, 2)),
        ],
        compiler_params=pltpu.CompilerParams(
            collective_id=0, has_side_effects=True, vmem_limit_bytes=58 * 2**20
        ),
    )(residual, gains, rel_bias, w_query, w_key, w_value, w_out)
    return staged


def solution(mesh):
    return jax.shard_map(
        functools.partial(on_device, mesh.shape["tp"], mesh.shape["sp"]),
        mesh=mesh,
        in_specs=(
            P("sp", "tp"),
            P(),
            P(None, None, "tp"),
            P(None, None, "tp"),
            P(None, None, "tp"),
            P(None, None, "tp"),
            P(None, "tp", None),
        ),
        out_specs=P("sp", "tp"),
        check_vma=False,
    )
```

```python
import functools

import jax
import jax.numpy as jnp
from jax import lax
from jax.experimental import pallas as pl
from jax.experimental.pallas import tpu as pltpu
from jax.sharding import PartitionSpec as P

HEAD = 64
SEG = 64
LEFT = 8
MAXREL = 128
BLOCK = 128
EPS = 1e-06
LOG2E = 1.4426950408889634
NEG = -1e30
SENT = 1
MESH = pl.DeviceIdType.MESH
F32 = jnp.float32
BF16 = jnp.bfloat16


def remote(src, dst, send_sem, recv_sem, where):
    return pltpu.make_async_remote_copy(
        src_ref=src,
        dst_ref=dst,
        send_sem=send_sem,
        recv_sem=recv_sem,
        device_id=where,
        device_id_type=MESH,
    )


def kernel(
    tp,
    sp_count,
    res_ref,
    gains_hbm,
    bias_hbm,
    wq_ref,
    wk_ref,
    wv_ref,
    wo_ref,
    out_ref,
    wbuf,
    gather,
    before,
    kbuf,
    vbuf,
    qbuf,
    branch,
    toeplitz,
    sums,
    gains_ref,
    bias_ref,
    held_sum,
    held_value,
    w_sem,
    io_sem,
    g_send,
    g_recv,
    f_send,
    b_send,
    b_recv,
    bf_send,
    h_send,
    h_recv,
):
    layers = wbuf.shape[0]
    tokens, cols = res_ref.shape
    width = cols * tp
    chunks = tokens // BLOCK
    pairs = cols // 128
    reach = LEFT * SEG
    blocks = reach // BLOCK
    me = lax.axis_index("tp")
    sp = lax.axis_index("sp")
    core = lax.rem(me, 2)
    sibling = me + 1 - 2 * core
    ychips = tp // 2
    first = sp == 0
    last = sp == sp_count - 1

    weights = (wq_ref, wk_ref, wv_ref, wo_ref)

    def weight_copy(l, k):
        return pltpu.make_async_copy(weights[k].at[l], wbuf.at[l, k], w_sem.at[l, k])

    def rows_of(c):
        return pl.ds(pl.multiple_of(c * BLOCK, BLOCK), BLOCK)

    def res_copy(c):
        return pltpu.make_async_copy(
            res_ref.at[rows_of(c)], gather.at[0, 0, me, rows_of(c)], io_sem.at[c]
        )

    gains_copy = pltpu.make_async_copy(gains_hbm, gains_ref, io_sem.at[chunks])
    bias_copy = pltpu.make_async_copy(bias_hbm, bias_ref, io_sem.at[chunks + 1])

    for c in reversed(range(chunks)):
        res_copy(c).start()
    bias_copy.start()
    gains_copy.start()
    for k in (1, 2, 0):
        weight_copy(0, k).start()

    barrier = pltpu.get_barrier_semaphore()
    for k in range(1, tp):
        pl.semaphore_signal(
            barrier, inc=1, device_id={"tp": lax.rem(me + k, tp)}, device_id_type=MESH
        )

    @pl.when(~first)
    def _():
        pl.semaphore_signal(
            barrier, inc=1, device_id={"sp": jnp.maximum(sp - 1, 0)}, device_id_type=MESH
        )

    pl.semaphore_wait(barrier, jnp.where(last, tp - 1, tp))

    def block_of(kind, l, c, slot, lanes=slice(None)):
        return gather.at[kind, l, slot, rows_of(c), lanes]

    def direct(kind, l, c, peer, source, lanes=slice(None)):
        ref = block_of(kind, l, c, source, lanes)
        way = jnp.where(peer == sibling, ychips - 1, lax.rem(peer // 2 + ychips - me // 2, ychips) - 1)
        return remote(ref, ref, g_send.at[c, way], g_recv.at[kind, c, source], {"tp": peer})

    def forward(kind, l, c, source):
        ref = block_of(kind, l, c, source)
        return remote(
            ref, ref, f_send.at[c, source // 2], g_recv.at[kind, c, source], {"tp": sibling}
        )

    def others(base):
        return [lax.rem(base + 2 * k, tp) for k in range(1, ychips)]

    def spread(kind, l, c, lanes=slice(None)):
        for peer in others(me):
            direct(kind, l, c, peer, me, lanes).start()
        direct(kind, l, c, sibling, me, lanes).start()

    def relay(kind, l, c):
        for source in others(me):
            direct(kind, l, c, source, source).wait_recv()
            forward(kind, l, c, source).start()

    def arrive(kind, l, c):
        direct(kind, l, c, sibling, sibling).wait_recv()
        for source in others(sibling):
            direct(kind, l, c, sibling, source).wait_recv()
        sent(kind, l, c)

    def sent(kind, l, c):
        for source in others(me):
            forward(kind, l, c, source).wait_send()
            direct(kind, l, c, source, me).wait_send()
        direct(kind, l, c, sibling, me).wait_send()

    def pass_on(l, c, source):
        return remote(
            block_of(0, l, c, source),
            before.at[l, source, rows_of(c - SENT)],
            b_send.at[c - SENT, source // 2],
            b_recv.at[l, c - SENT, source],
            {"sp": lax.rem(sp + 1, sp_count)},
        )

    def pass_across(l, c, source):
        ref = before.at[l, source, rows_of(c - SENT)]
        return remote(
            ref,
            ref,
            bf_send.at[c - SENT, source // 2],
            b_recv.at[l, c - SENT, source],
            {"tp": sibling},
        )

    def relay_stream(l, c):
        relay(0, l, c)

        @pl.when((c >= SENT) & ~last)
        def _():
            for source in others(me):
                pass_on(l, c, source).start()

        @pl.when((c == jnp.where(l == 0, chunks - 2, chunks - 1)) & ~last)
        def _():
            for held in reversed(range(SENT, chunks - 2)):
                pass_on(l, held, me).start()

    def update(l, parts):
        old, branches = parts
        branches = [part.astype(F32) for part in branches]
        total = sum(jnp.sum(part * part, axis=1, keepdims=True) for part in branches)
        inv = lax.rsqrt(total / width + EPS)
        gain = gains_ref[l - 1, 1:2, :]
        return [
            (part.astype(F32) + b * inv * gain[:, j * cols : (j + 1) * cols]).astype(BF16)
            for j, (part, b) in enumerate(zip(old, branches))
        ]

    def relay_before(l, c, sources):
        @pl.when(~first)
        def _():
            for source in sources:
                pass_on(l, c, source).wait_recv()
                pass_across(l, c, source).start()

    def halo(l, c, which):
        if which == 0:
            src, dst = kbuf.at[l, rows_of(c + blocks)], kbuf.at[l, rows_of(c)]
        else:
            src, dst = vbuf.at[l, c + blocks], vbuf.at[l, c]
        return remote(
            src,
            dst,
            h_send.at[c, which],
            h_recv.at[l, c, which],
            {"sp": lax.rem(sp + 1, sp_count)},
        )

    def sum_copies(c):
        pairs_of = [(peer, g_send.at[c, k]) for k, peer in enumerate(others(me))]
        pairs_of.append((sibling, g_send.at[c, ychips - 1]))
        pairs_of += [(peer, f_send.at[c, k]) for k, peer in enumerate(others(sibling))]

        def copy(peer, source, sem):
            ref = sums.at[c, source]
            return remote(ref, ref, sem, g_recv.at[0, c, source], {"tp": peer})

        return [(copy(peer, me, sem), copy(peer, peer, sem)) for peer, sem in pairs_of]

    for c in reversed(range(chunks)):
        res_copy(c).wait()
        spread(0, 0, c)
        if c >= max(SENT, chunks - 2):

            @pl.when(~last)
            def _():
                pass_on(0, c, me).start()

    @pl.when(first)
    def _():
        for l in range(layers):
            kbuf[l, :reach] = jnp.zeros((reach, cols), BF16)
            vbuf[l, :blocks] = jnp.zeros((blocks, cols, BLOCK), BF16)

    row = lax.broadcasted_iota(jnp.int32, (BLOCK, BLOCK), 0)
    col = lax.broadcasted_iota(jnp.int32, (BLOCK, BLOCK), 1)
    low = col < HEAD
    late = jnp.where((row >= SEG) & (col < SEG), NEG, 0.0).astype(F32)
    place = lax.broadcasted_iota(jnp.int32, (1, 2 * BLOCK), 1)
    early = jnp.where(lax.rem(place, BLOCK) >= SEG, NEG, 0.0).astype(F32)

    def scaled_and_inv(l, parts):
        parts = [part.astype(F32) for part in parts]
        gain = gains_ref[l, 0:1, :]
        scaled = jnp.concatenate(
            [
                (part * gain[:, j * cols : (j + 1) * cols]).astype(BF16)
                for j, part in enumerate(parts)
            ],
            axis=1,
        )
        total = sum(jnp.sum(part * part, axis=1, keepdims=True) for part in parts)
        return scaled, lax.rsqrt(total / width + EPS)

    def store_keys_values(l, slot, scaled, inv):
        value = jnp.dot(scaled, wbuf[l, 2], preferred_element_type=F32)
        vbuf[l, slot] = (value * inv).T.astype(BF16)
        key = jnp.dot(scaled, wbuf[l, 1], preferred_element_type=F32)
        kbuf[l, rows_of(slot)] = (key * inv).astype(BF16)

    def partial_keys_values(c, sources):
        sums_of = values = keys = None
        for source in sources:
            part = gather[0, 0, source, rows_of(c)].astype(F32)
            at = pl.ds(pl.multiple_of(source * cols, cols), cols)
            scaled = (part * gains_ref[0, 0:1, at]).astype(BF16)
            square = jnp.sum(part * part, axis=1, keepdims=True)
            value = jnp.dot(scaled, wbuf[0, 2, at], preferred_element_type=F32)
            key = jnp.dot(scaled, wbuf[0, 1, at], preferred_element_type=F32)
            sums_of = square if sums_of is None else sums_of + square
            values = value if values is None else values + value
            keys = key if keys is None else keys + key
        return sums_of, values, keys

    def project(l, c):
        rows = rows_of(c)

        @pl.when(l == 0)
        def _():
            direct(0, 0, c, sibling, sibling).wait_recv()
            square, values, keys = partial_keys_values(c, [me, sibling] + others(me))
            held_sum[...] = jnp.broadcast_to(square, held_sum.shape)
            held_value[0] = values
            held_value[1] = keys
            for source in others(sibling):
                direct(0, 0, c, sibling, source).wait_recv()
            sent(0, 0, c)
            square, values, keys = partial_keys_values(c, others(sibling))
            inv = lax.rsqrt((held_sum[:, 0:1] + square) / width + EPS)
            vbuf[0, c + blocks] = ((held_value[0] + values) * inv).T.astype(BF16)
            kbuf[0, rows_of(c + blocks)] = ((held_value[1] + keys) * inv).astype(BF16)

        pl.when(l > 0)(lambda: arrive(0, l, c))

        @pl.when(l > 0)
        def _():
            own = ([gather[0, k, j, rows] for j in range(tp)] for k in (0, l))
            parts = update(l, own)
            for j, part in enumerate(parts):
                gather[0, 0, j, rows] = part
            store_keys_values(l, c + blocks, *scaled_and_inv(l, parts))


        @pl.when((c < SENT) & ~last)
        def _():
            halo(l, c, 0).start()
            halo(l, c, 1).start()

    def ask(l, c):
        rows = rows_of(c)
        scaled, inv = scaled_and_inv(l, [gather[0, 0, j, rows] for j in range(tp)])
        query = jnp.dot(scaled, wbuf[l, 0], preferred_element_type=F32)
        qbuf[rows] = (query * (inv * (LOG2E * HEAD**-0.5))).astype(BF16)

    def project_before(l, c):
        @pl.when(~first)
        def _():
            for source in [sibling] + others(sibling):
                pass_across(l, c, source).wait_recv()
            for source in [me] + others(me):
                pass_across(l, c, source).wait_send()
            rows = rows_of(c - SENT)

            @pl.when(l > 0)
            def _():
                halo_parts = ([before[k, j, rows] for j in range(tp)] for k in (0, l))
                parts = update(l, halo_parts)
                for j, part in enumerate(parts):
                    before[0, j, rows] = part
                store_keys_values(l, c, *scaled_and_inv(l, parts))

            @pl.when(l == 0)
            def _():
                parts = [before[0, j, rows] for j in range(tp)]
                store_keys_values(l, c, *scaled_and_inv(l, parts))

    def attention(l, c):
        @pl.when((c < SENT) & ~first)
        def _():
            halo(l, c, 0).wait_recv()
            halo(l, c, 1).wait_recv()

        window = pl.ds(pl.multiple_of(c * BLOCK, BLOCK), reach + BLOCK)
        closed = [
            jnp.where(first & (c + i < blocks), NEG, 0.0).astype(F32) for i in range(blocks)
        ]

        def score(pair):
            lanes = slice(pair * 128, (pair + 1) * 128)
            query = qbuf[rows_of(c), lanes]
            zero = jnp.zeros_like(query)
            both = jnp.concatenate(
                [jnp.where(low, query, zero), jnp.where(low, zero, query)], axis=0
            )
            scores = lax.dot_general(
                kbuf[l, window, lanes],
                both,
                (((1,), (1,)), ((), ())),
                preferred_element_type=F32,
            )
            tiles = []
            tops = []
            for i in range(blocks + 1):
                tile = scores[i * BLOCK : (i + 1) * BLOCK]
                if i == 0:
                    tile = jnp.concatenate([tile[:SEG] + early, tile[SEG:]], axis=0)
                if i >= blocks - 1:
                    tile = tile + toeplitz[l, pair, i - blocks + 1]
                top = jnp.max(tile.reshape(BLOCK // 8, 8, 2 * BLOCK), axis=0)
                if i < blocks:
                    top = top + closed[i]
                tiles.append(tile)
                tops.append(top)
            return tiles, jnp.max(functools.reduce(jnp.maximum, tops), axis=0, keepdims=True)

        def mix(pair, tiles, top):
            lanes = slice(pair * 128, (pair + 1) * 128)
            raw = []
            parts = []
            for i in range(blocks + 1):
                tile = jnp.exp2(tiles[i] - (top - closed[i] if i < blocks else top))
                parts.append(jnp.sum(tile.reshape(BLOCK // 8, 8, 2 * BLOCK), axis=0))
                raw.append(tile.astype(BF16))
            total = jnp.sum(functools.reduce(jnp.add, parts), axis=0, keepdims=True)
            values = jnp.concatenate([vbuf[l, c + i, lanes] for i in range(blocks + 1)], axis=1)
            mixed = jnp.dot(values, jnp.concatenate(raw, axis=0), preferred_element_type=F32)
            mixed = mixed * (1.0 / total)
            mixed = jnp.concatenate([mixed[:HEAD, :BLOCK], mixed[HEAD:, BLOCK:]], axis=0)
            gather[1, l, me, rows_of(c), lanes] = mixed.T.astype(BF16)

        held = [score(pair) for pair in range(pairs)]
        for pair in range(pairs):
            mix(pair, *held[pair])
            if pair == pairs // 2 - 1:
                spread(1, l, c, slice(0, (pair + 1) * 128))
        spread(1, l, c, slice(pairs // 2 * 128, cols))

    def out_product(l, c):
        arrive(1, l, c)
        whole = jnp.concatenate([gather[1, l, j, rows_of(c)] for j in range(tp)], axis=1)
        return jnp.dot(whole, wbuf[l, 3], preferred_element_type=F32)

    def hand_on(l, c):
        later = jnp.minimum(l + 1, layers - 1)
        gather[0, later, me, rows_of(c)] = out_product(l, c).astype(BF16)
        spread(0, later, c)

        @pl.when((c >= max(SENT, chunks - 2)) & ~last)
        def _():
            pass_on(later, c, me).start()

    def out_project(l, c):
        def product(sources):
            total = None
            for source in sources:
                rows = pl.ds(pl.multiple_of(source * cols, cols), cols)
                part = jnp.dot(
                    gather[1, l, source, rows_of(c)],
                    wbuf[l, 3, rows],
                    preferred_element_type=F32,
                )
                total = part if total is None else total + part
            return total

        direct(1, l, c, sibling, sibling).wait_recv()
        branch[rows_of(c)] = product([me, sibling] + others(me))
        for source in others(sibling):
            direct(1, l, c, sibling, source).wait_recv()
        sent(1, l, c)
        value = branch[rows_of(c)] + product(others(sibling))
        branch[rows_of(c)] = value
        square = jnp.sum(value * value, axis=1, keepdims=True)
        sums[c, me] = jnp.broadcast_to(square, (BLOCK, BLOCK)).T[:8]
        for mine, _ in sum_copies(c):
            mine.start()

    def finish(c):
        for mine, theirs in sum_copies(c):
            theirs.wait_recv()
            mine.wait_send()
        total = functools.reduce(jnp.add, [sums[c, j] for j in range(tp)])
        inv = lax.rsqrt(total / width + EPS)
        inv = jnp.broadcast_to(inv[0:1], (BLOCK, BLOCK)).T[:, 0:1]
        gain = gains_ref[layers - 1, 1:2, pl.ds(pl.multiple_of(me * cols, 128), cols)]
        new = gather[0, 0, me, rows_of(c)].astype(F32) + branch[rows_of(c)] * inv * gain
        out_ref[rows_of(c)] = new.astype(BF16)

    def passed_on(l):
        @pl.when(~last)
        def _():
            for c in range(chunks):
                if c < SENT:
                    halo(l, c, 0).wait_send()
                    halo(l, c, 1).wait_send()
                else:
                    for source in [me] + others(me):
                        pass_on(l, c, source).wait_send()

    def tables(l, carry):
        far = bias_ref[l, :, 2 * MAXREL :]
        near = (bias_ref[l, :, : 2 * MAXREL] - far) * LOG2E
        for h in range(2 * pairs):
            line = jnp.concatenate([jnp.zeros((1, BLOCK), F32), near[h : h + 1]], axis=1)
            line = jnp.broadcast_to(line, (2 * BLOCK, 3 * BLOCK))
            skewed = pltpu.roll(line, 0, 1, stride=1, stride_axis=0)
            at = slice(h % 2 * BLOCK, (h % 2 + 1) * BLOCK)
            toeplitz[l, h // 2, 0, :, at] = skewed[:BLOCK, :BLOCK]
            toeplitz[l, h // 2, 1, :, at] = skewed[BLOCK:, :BLOCK] + late
        return carry

    bias_copy.wait()
    lax.fori_loop(0, layers, tables, 0)
    gains_copy.wait()

    def closing(t, carry):
        finish(chunks - 1 - t)
        return carry

    period = 2 * chunks

    def step(g, carry):
        def stage(lag, count=chunks):
            index = g - lag
            l = jnp.clip(index // period, 0, layers - 1)
            t = index - l * period
            return (t >= 0) & (t < count), l, chunks - 1 - t

        def on(lag, count=chunks, extra=True):
            live, l, c = stage(lag, count)
            return lambda run: pl.when(live & extra)(lambda: run(l, c))

        def layer_at(lag):
            return jnp.clip((g - lag) // period, 0, layers - 1)

        def relay_rest(l, c):
            pl.when((c >= SENT) & (c < chunks - 2))(lambda: relay_before(l, c, [me]))
            pl.when(c >= SENT)(lambda: relay_before(l, c, others(me)))

        on(0)(relay_stream)
        on(1, 2)(lambda l, c: relay_before(l, c, [me]))
        live, l, c = stage(1, 2)
        pl.when(live & (c == jnp.where(l == 0, chunks - 2, chunks - 1)))(
            lambda: relay_rest(l, chunks - 1)
        )
        before_live, before_l, c = stage(chunks - 2, chunks - SENT + 1)
        u = chunks - 1 - c
        before_c = jnp.where(u == 0, chunks - 1, chunks - u)
        pl.when(before_live & (u != jnp.where(before_l == 0, 0, 1)))(
            lambda: project_before(before_l, before_c)
        )

        @pl.when(g == 0)
        def _():
            for k in (1, 2, 0):
                weight_copy(0, k).wait()
            weight_copy(0, 3).start()

        @pl.when((g > 0) & (lax.rem(g, period) == 0) & (g < layers * period))
        def _():
            for k in (1, 2, 0, 3):
                weight_copy(layer_at(0), k).wait()

        ask_live, ask_l, c = stage(1, 3)
        v = chunks - 1 - c

        @pl.when(ask_live & ((v == 0) | (v == jnp.where(ask_l == 0, 1, 2))))
        def _():
            first_c = chunks - 1 - jnp.minimum(v, 1)

            def one(i, carry):
                ask(ask_l, first_c - i)
                return carry

            lax.fori_loop(0, jnp.where(v == 2, 2, 1), one, 0)

        on(0)(project)
        on(chunks - 1, 1)(lambda l, c: relay_rest(l, c - 1))

        @pl.when((lax.rem(g, period) == 1) & (g < (layers - 1) * period))
        def _():
            for k in (1, 2, 0, 3):
                weight_copy(jnp.minimum(layer_at(0) + 1, layers - 1), k).start()

        on(chunks + 2, chunks, layer_at(chunks + 2) == layers - 1)(lambda l, c: relay(1, l, c))
        on(chunks - 1)(attention)
        on(chunks + 1, chunks, layer_at(chunks + 1) < layers - 1)(lambda l, c: relay(1, l, c))
        rest_live, rest_l, rest_c = stage(chunks, 2)
        pl.when(rest_live & ((rest_l == 0) | (rest_c == chunks - 2)))(
            lambda: ask(rest_l, rest_c - chunks + 2)
        )
        on(chunks - 1, chunks - SENT - 2, layer_at(chunks - 1) > 0)(lambda l, c: relay_rest(l, c - 2))
        on(chunks, chunks - SENT - 2, layer_at(chunks) == 0)(lambda l, c: relay_rest(l, c - 2))

        @pl.when(g == chunks + 1)
        def _():
            weight_copy(0, 3).wait()

        on(chunks + 1, 1)(lambda l, c: passed_on(l))
        on(chunks + 1, chunks, layer_at(chunks + 1) < layers - 1)(hand_on)
        on(chunks + 2, chunks, layer_at(chunks + 2) == layers - 1)(out_project)
        return carry

    lax.fori_loop(0, (layers - 1) * period + 2 * chunks + 2, step, 0)
    lax.fori_loop(0, chunks, closing, 0)


def on_device(tp, sp_count, residual, gains, w_query, w_key, w_value, w_out, rel_bias):
    tokens, cols = residual.shape
    layers, width, _ = w_query.shape
    chunks = tokens // BLOCK
    reach = LEFT * SEG
    pairs = cols // 128
    ychips = tp // 2
    hbm = pl.BlockSpec(memory_space=pl.ANY)
    dma = pltpu.SemaphoreType.DMA
    staged = pl.pallas_call(
        functools.partial(kernel, tp, sp_count),
        out_shape=pltpu.VMEM((tokens, cols), BF16),
        in_specs=[hbm] * 7,
        out_specs=pl.BlockSpec(memory_space=pltpu.VMEM),
        scratch_shapes=[
            pltpu.VMEM((layers, 4, width, cols), BF16),
            pltpu.VMEM((2, layers, tp, tokens, cols), BF16),
            pltpu.VMEM((layers, tp, tokens - SENT * BLOCK, cols), BF16),
            pltpu.VMEM((layers, reach + tokens, cols), BF16),
            pltpu.VMEM((layers, reach // BLOCK + chunks, cols, BLOCK), BF16),
            pltpu.VMEM((tokens, cols), BF16),
            pltpu.VMEM((tokens, cols), F32),
            pltpu.VMEM((layers, pairs, 2, BLOCK, 2 * BLOCK), F32),
            pltpu.VMEM((chunks, tp, 8, BLOCK), F32),
            pltpu.VMEM(gains.shape, F32),
            pltpu.VMEM(rel_bias.shape, F32),
            pltpu.VMEM((BLOCK, 128), F32),
            pltpu.VMEM((2, BLOCK, cols), F32),
            dma((layers, 4)),
            dma((chunks + 2,)),
            dma((chunks, ychips)),
            dma((2, chunks, tp)),
            dma((chunks, ychips)),
            dma((chunks - SENT, ychips)),
            dma((layers, chunks - SENT, tp)),
            dma((chunks - SENT, ychips)),
            dma((SENT, 2)),
            dma((layers, SENT, 2)),
        ],
        compiler_params=pltpu.CompilerParams(
            collective_id=0, has_side_effects=True, vmem_limit_bytes=58 * 2**20
        ),
    )(residual, gains, rel_bias, w_query, w_key, w_value, w_out)
    return staged


def solution(mesh):
    return jax.shard_map(
        functools.partial(on_device, mesh.shape["tp"], mesh.shape["sp"]),
        mesh=mesh,
        in_specs=(
            P("sp", "tp"),
            P(),
            P(None, None, "tp"),
            P(None, None, "tp"),
            P(None, None, "tp"),
            P(None, None, "tp"),
            P(None, "tp", None),
        ),
        out_specs=P("sp", "tp"),
        check_vma=False,
    )
```
